32 devices in a mesh: sp: 8 (over z, y), tp: 4 (over x, core).
Axes of the slice: x: 2, y: 2, z: 4, core: 2. Of those that a mesh axis runs over, the one named last changes fastest.
Arguments:
- queries_one: bfloat16 [2048, 512], P('sp', 'tp'), may hold values from -6 to 6
- queries_two: bfloat16 [2048, 512], P('sp', 'tp'), may hold values from -6 to 6
- keys_one: bfloat16 [2048, 512], P('sp', 'tp'), may hold values from -6 to 6
- keys_two: bfloat16 [2048, 512], P('sp', 'tp'), may hold values from -6 to 6
- values: bfloat16 [2048, 1024], P('sp', 'tp'), may hold values from -6 to 6
- mix_lambda: float32 [4], P('tp'), may hold values from 0.3 to 0.8
- head_gain: float32 [1024], P('tp'), may hold values from 0.1 to 1.9
- out_weight: bfloat16 [1024, 2048], P('tp'), may hold values from -0.1875 to 0.1875
- residual_in: bfloat16 [2048, 2048], P('sp', 'tp'), may hold values from -12 to 12
- norm_gain: float32 [2048], replicated, may hold values from 0.1 to 1.9
- gate_weight: bfloat16 [2048, 5632], P('sp', 'tp'), may hold values from -0.125 to 0.125
- up_weight: bfloat16 [2048, 5632], P('sp', 'tp'), may hold values from -0.125 to 0.125
- down_weight: bfloat16 [5632, 2048], P('tp', 'sp'), may hold values from -0.078125 to 0.078125
Outputs:
- layer_out: bfloat16 [2048, 2048], P('sp', 'tp')
The draws below stay inside these ranges and needn't reach their ends.
All inputs are finite; a program needn't handle non-finite values.
Results may differ from the reference program's by a relative error of at most 0.012.
Values may be sent and summed in bfloat16 or wider, within the bound.
A program may use at most 192 MiB of HBM per device.

```python
import math
import jax
import jax.numpy as jnp
from jax import lax

D = 2048
HEADS = 4
HEAD = 128
VALUE = 256
FF = 5632
SEQ = 2048
N_TP = 4


def planted(key, salt, pattern_salt, query_side):
    columns = HEADS * HEAD
    noise = 1.3 * jax.random.normal(jax.random.fold_in(key, salt), (SEQ, columns), jnp.float32)
    noise = jnp.clip(noise, -6.0, 6.0)
    return noise.astype(jnp.bfloat16)


def draw_queries_one(key, part):
    return planted(key, 1, 71, True)


def draw_keys_one(key, part):
    return planted(key, 2, 71, False)


def draw_queries_two(key, part):
    return planted(key, 3, 72, True)


def draw_keys_two(key, part):
    return planted(key, 4, 72, False)


def draw_residual_in(key, part):
    order = jax.random.permutation(jax.random.fold_in(key, 11), 4)
    column = jnp.arange(D, dtype=jnp.int32)
    quarter = column * 4 // D
    level = order[quarter].astype(jnp.float32)
    scales = 0.4 + 0.55 * level
    noise = jax.random.normal(jax.random.fold_in(key, 12), (SEQ, D), jnp.float32) * scales[None, :]
    return jnp.clip(noise, -12.0, 12.0).astype(jnp.bfloat16)


def shard_levels(own_key, shape, cuts, least, top_value):
    def one(position, blocks):
        steps = jax.random.uniform(jax.random.fold_in(jax.random.fold_in(own_key, 6), position), (blocks,), jnp.float32, least / len(cuts), top_value / len(cuts))
        return jnp.repeat(jnp.exp(steps), shape[position] // blocks).reshape((-1,) + (1,) * (len(shape) - position - 1))

    gain = one(*cuts[0])
    for cut in cuts[1:]:
        gain = gain * one(*cut)
    return gain


def scatter_about(key, extent, scale, bound, cuts=(), kind=jnp.bfloat16):
    drawn = jax.random.normal(key, extent, jnp.float32) * scale
    if len(cuts) > 0:
        drawn = shard_levels(key, extent, cuts, -0.22, 0.18) * drawn
    return jnp.clip(drawn, min=-bound, max=bound).astype(kind)


def setup_inputs(seed: int = 0) -> dict:
    keys = jax.random.split(jax.random.key(seed), 14)
    return {
        "queries_one": draw_queries_one(jax.random.fold_in(keys[13], 71), 0),
        "queries_two": draw_queries_two(jax.random.fold_in(keys[13], 71), 0),
        "keys_one": draw_keys_one(jax.random.fold_in(keys[13], 71), 0),
        "keys_two": draw_keys_two(jax.random.fold_in(keys[13], 71), 0),
        "values": scatter_about(keys[4], (SEQ, HEADS * VALUE), 1.0, 6.0, ((0, 8), (1, 4))),
        "mix_lambda": jnp.clip(0.3 + 0.5 * jax.random.uniform(keys[5], (HEADS,), jnp.float32) ** shard_levels(keys[5], (HEADS,), ((0, 4),), -0.2, 0.2), 0.3, 0.8),
        "head_gain": jnp.clip(1.0 + 0.18 * jax.random.normal(keys[6], (HEADS * VALUE,), jnp.float32), 0.1, 1.9),
        "out_weight": scatter_about(keys[7], (HEADS * VALUE, D), (HEADS * VALUE) ** -0.5, 0.1875, ((0, 4),)),
        "residual_in": draw_residual_in(jax.random.fold_in(keys[13], 71), 0),
        "norm_gain": jnp.clip(1.0 + 0.18 * jax.random.normal(keys[9], (D,), jnp.float32), 0.1, 1.9),
        "gate_weight": scatter_about(keys[10], (D, FF), D ** -0.5, 0.125, ((0, 8), (1, 4))),
        "up_weight": scatter_about(keys[11], (D, FF), D ** -0.5, 0.125, ((0, 8), (1, 4))),
        "down_weight": scatter_about(keys[12], (FF, D), FF ** -0.5, 0.078125, ((0, 4), (1, 8))),
    }


epsilon = 1e-06

def head_maps(query_one, query_two, key_one, key_two, value_rows, lam_head):
    seq_len = query_one.shape[0]
    block_rows = math.gcd(seq_len, 512)
    score_scale = HEAD ** (-0.5)
    key_pos = jnp.arange(seq_len, dtype=jnp.int32)

    def one_block(block_index):
        first_row = (block_index * block_rows).astype(jnp.int32)
        query_pos = first_row + jnp.arange(block_rows, dtype=jnp.int32)
        visible = key_pos[None, :] <= query_pos[:, None]

        def one_map(queries, key_rows):
            picked = lax.dynamic_slice_in_dim(queries, first_row, block_rows, 0)
            scores = jnp.dot(picked, key_rows.T, preferred_element_type=jnp.float32) * score_scale
            scores = jnp.where(visible, scores, -jnp.inf)
            highest = lax.optimization_barrier(jnp.max(scores, axis=1, keepdims=True))
            weights_exp = jnp.exp(scores - highest)
            totals = lax.optimization_barrier(jnp.sum(weights_exp, axis=1, keepdims=True))
            return jnp.dot(weights_exp.astype(jnp.bfloat16), value_rows, preferred_element_type=jnp.float32) / totals
        return one_map(query_one, key_one) - lam_head * one_map(query_two, key_two)
    blocks = lax.map(one_block, jnp.arange(seq_len // block_rows, dtype=jnp.int32))
    return blocks.reshape(seq_len, VALUE)

def rounded_sum(left, right, groups):
    width = left.shape[1] // groups
    result = jnp.zeros((left.shape[0], right.shape[1]), jnp.float32)
    for group in range(groups):
        partial_bf = jnp.dot(left[:, group * width:(group + 1) * width], right[group * width:(group + 1) * width], preferred_element_type=jnp.float32).astype(jnp.bfloat16)
        partial_bf = lax.optimization_barrier(partial_bf)
        result = result + partial_bf.astype(jnp.float32)
    return result

def reference(queries_one, queries_two, keys_one, keys_two, values, mix_lambda, head_gain, out_weight, residual_in, norm_gain, gate_weight, up_weight, down_weight):
    pieces = []
    for head_index in range(HEADS):
        qcols = slice(head_index * HEAD, (head_index + 1) * HEAD)
        vcols = slice(head_index * VALUE, (head_index + 1) * VALUE)
        mixed = head_maps(queries_one[:, qcols], queries_two[:, qcols], keys_one[:, qcols], keys_two[:, qcols], values[:, vcols], mix_lambda[head_index])
        mean_square = lax.optimization_barrier(jnp.mean(mixed * mixed, axis=1, keepdims=True))
        normed_head = mixed * lax.rsqrt(mean_square + epsilon) * head_gain[vcols][None, :] * 0.8
        pieces.append(normed_head.astype(jnp.bfloat16))
    attended = jnp.concatenate(pieces, axis=1)
    projected = rounded_sum(attended, out_weight, N_TP)
    resid = (residual_in.astype(jnp.float32) + projected).astype(jnp.bfloat16)
    resid_float = resid.astype(jnp.float32)
    mean_square = lax.optimization_barrier(jnp.mean(resid_float * resid_float, axis=1, keepdims=True))
    normed = (resid_float * lax.rsqrt(mean_square + epsilon) * norm_gain[None, :]).astype(jnp.bfloat16)
    gate_act = jnp.dot(normed, gate_weight, preferred_element_type=jnp.float32)
    up_act = jnp.dot(normed, up_weight, preferred_element_type=jnp.float32)
    hidden = (jax.nn.silu(gate_act) * up_act).astype(jnp.bfloat16)
    mlp_out = rounded_sum(hidden, down_weight, N_TP)
    return (resid_float + mlp_out).astype(jnp.bfloat16)
```

```python
import functools

import jax
import jax.numpy as jnp
from jax import lax
from jax.experimental import pallas as pl
from jax.experimental.pallas import tpu as pltpu
from jax.sharding import PartitionSpec as P

HEAD = 128


epsilon = 1e-06
masked_score = -1e30


def per_device(
    queries_one,
    queries_two,
    keys_one,
    keys_two,
    values,
    mix_lambda,
    head_gain,
    out_weight,
    residual_in,
    norm_gain,
    gate_weight,
    up_weight,
    down_weight,
):
    tok_rows = queries_one.shape[0]
    heads_here = mix_lambda.shape[0]
    head_width = HEAD
    value_width = values.shape[1] // heads_here
    query_pos = lax.axis_index("sp") * tok_rows + jnp.arange(tok_rows, dtype=jnp.int32)
    query_first = queries_one.reshape(tok_rows, heads_here, head_width)
    query_second = queries_two.reshape(tok_rows, heads_here, head_width)
    score_scale = head_width ** (-0.5)

    def update(state, queries, key_rows, value_rows, visible):
        running, totals, weighted = state
        scores = (
            jnp.einsum("qhd,khd->hqk", queries, key_rows, preferred_element_type=jnp.float32)
            * score_scale
        )
        scores = jnp.where(visible[None], scores, masked_score)
        highest = jnp.maximum(running, jnp.max(scores, axis=2))
        weights_exp = jnp.where(visible[None], jnp.exp(scores - highest[..., None]), 0.0)
        totals = jnp.sum(weights_exp, axis=2)
        weighted = jnp.einsum(
            "hqk,khd->hqd",
            weights_exp.astype(jnp.bfloat16),
            value_rows,
            preferred_element_type=jnp.float32,
        )
        return (highest, totals, weighted)

    initial = (
        jnp.full((heads_here, tok_rows), masked_score, jnp.float32),
        jnp.zeros((heads_here, tok_rows), jnp.float32),
        jnp.zeros((heads_here, tok_rows, value_width), jnp.float32),
    )
    key_first = lax.all_gather(keys_one, "sp", axis=0, tiled=True)
    key_second = lax.all_gather(keys_two, "sp", axis=0, tiled=True)
    value_piece = lax.all_gather(values, "sp", axis=0, tiled=True)
    key_count = key_first.shape[0]
    key_pos = jnp.arange(key_count, dtype=jnp.int32)
    visible = key_pos[None, :] <= query_pos[:, None]
    value_rows = value_piece.reshape(key_count, heads_here, value_width)
    first_new = update(
        initial,
        query_first,
        key_first.reshape(key_count, heads_here, head_width),
        value_rows,
        visible,
    )
    second_new = update(
        initial,
        query_second,
        key_second.reshape(key_count, heads_here, head_width),
        value_rows,
        visible,
    )
    lam_heads = mix_lambda[:, None, None]
    mixed = (
        first_new[2] / first_new[1][..., None]
        - lam_heads * second_new[2] / second_new[1][..., None]
    )
    mean_square = jnp.mean(mixed * mixed, axis=2, keepdims=True)
    normed_heads = (
        mixed
        * lax.rsqrt(mean_square + epsilon)
        * head_gain.reshape(heads_here, 1, value_width)
        * 0.8
    )
    attended = (
        normed_heads.transpose(1, 0, 2)
        .reshape(tok_rows, heads_here * value_width)
        .astype(jnp.bfloat16)
    )
    projected = lax.psum_scatter(
        lax.dot_general(
            out_weight, attended, (((0,), (1,)), ((), ())), preferred_element_type=jnp.float32
        ).astype(jnp.bfloat16),
        "tp",
        scatter_dimension=0,
        tiled=True,
    ).astype(jnp.float32)
    resid = (residual_in.astype(jnp.float32) + projected.T).astype(jnp.bfloat16)
    full_rows = lax.all_gather(resid, "tp", axis=1, tiled=True)
    full_float = full_rows.astype(jnp.float32)
    mean_rows = jnp.mean(full_float * full_float, axis=1, keepdims=True)
    normed = (full_float * lax.rsqrt(mean_rows + epsilon) * norm_gain[None, :]).astype(jnp.bfloat16)
    gate_act = jnp.dot(
        normed,
        lax.all_gather(gate_weight, "sp", axis=0, tiled=True),
        preferred_element_type=jnp.float32,
    )
    up_act = jnp.dot(
        normed,
        lax.all_gather(up_weight, "sp", axis=0, tiled=True),
        preferred_element_type=jnp.float32,
    )
    hidden = (jax.nn.silu(gate_act) * up_act).astype(jnp.bfloat16)
    partials = jnp.dot(
        hidden,
        lax.all_gather(down_weight, "sp", axis=1, tiled=True),
        preferred_element_type=jnp.float32,
    )
    mlp_out = lax.psum_scatter(
        partials.astype(jnp.bfloat16), "tp", scatter_dimension=1, tiled=True
    ).astype(jnp.float32)
    return (resid.astype(jnp.float32) + mlp_out).astype(jnp.bfloat16)


def remote(src, dst, send, recv, where):
    return pltpu.make_async_remote_copy(
        src_ref=src,
        dst_ref=dst,
        send_sem=send,
        recv_sem=recv,
        device_id=where,
        device_id_type=pl.DeviceIdType.MESH,
    )


def greet(peers):
    barrier = pltpu.get_barrier_semaphore()
    for where in peers:
        pl.semaphore_signal(
            barrier, inc=1, device_id=where, device_id_type=pl.DeviceIdType.MESH
        )
    pl.semaphore_wait(barrier, len(peers))


def neighbours(n_sp, n_tp):
    s, t = lax.axis_index("sp"), lax.axis_index("tp")
    y_peer = s + 1 - 2 * lax.rem(s, 2)
    sibling = t + 1 - 2 * lax.rem(t, 2)
    across = lax.rem(t + 2, n_tp)
    return s, t, y_peer, sibling, across


def spread_kernel(n_sp, n_tp, w_ref, kv_ref, wall, kvall, *sems):
    kv_s, kv_r, a_s, a_r, x_s, x_r, c_s, c_r, f_s, f_r, loc = sems
    s, t, _, sibling, across = neighbours(n_sp, n_tp)
    rows = kv_ref.shape[0]
    part = w_ref.shape[1] // n_sp
    depth = w_ref.shape[2]
    greet(
        [{"sp": lax.rem(s + i, n_sp)} for i in range(1, n_sp)]
        + [{"tp": sibling}, {"tp": across}]
    )

    def block(who, source):
        return wall.at[:, who, :, pl.ds(pl.multiple_of(source * depth, depth), depth)]

    def piece(dest):
        return w_ref.at[:, pl.ds(pl.multiple_of(dest * part, 16), part), :]

    pending = []
    kv_in, a_in = [], []
    mine = kvall.at[pl.ds(pl.multiple_of(s * rows, rows), rows), :]
    for i in range(1, n_sp):
        copy = remote(kv_ref, mine, kv_s.at[i - 1], kv_r.at[i - 1], {"sp": lax.rem(s + i, n_sp)})
        copy.start()
        kv_in.append(copy)
    for i in range(1, n_sp):
        p = lax.rem(s + i, n_sp)
        copy = remote(piece(p), block(t, s), a_s.at[i - 1], a_r.at[i - 1], {"sp": p})
        copy.start()
        a_in.append(copy)
    own_kv = pltpu.make_async_copy(kv_ref, mine, loc.at[0])
    own_kv.start()
    own_w = pltpu.make_async_copy(piece(s), block(t, s), loc.at[1])
    own_w.start()
    x_in, c_in, f_in = [], [], []

    def forward(i):
        source = lax.rem(s - i + n_sp, n_sp)
        remote(
            block(t, source), block(t, source), x_s.at[i], x_r.at[i], {"tp": across}
        ).wait_recv()
        copy = remote(
            block(across, source), block(across, source), f_s.at[i], f_r.at[i], {"tp": sibling}
        )
        copy.start()
        f_in.append(copy)

    for i in range(n_sp):
        source = lax.rem(s - i + n_sp, n_sp)
        if i == 0:
            own_w.wait()
        else:
            a_in[i - 1].wait_recv()
        for send, recv, where, into in ((x_s, x_r, across, x_in), (c_s, c_r, sibling, c_in)):
            copy = remote(
                block(t, source), block(t, source), send.at[i], recv.at[i], {"tp": where}
            )
            copy.start()
            into.append(copy)
        if i >= 1:
            forward(i - 1)
    forward(n_sp - 1)
    own_kv.wait()
    for copy in kv_in:
        copy.wait()
    for copy in a_in + x_in:
        copy.wait_send()
    for copy in c_in + f_in:
        copy.wait()


def spread(weights, kv, n_sp, n_tp):
    three, ff_here, depth = weights.shape
    dma = pltpu.SemaphoreType.DMA
    return pl.pallas_call(
        functools.partial(spread_kernel, n_sp, n_tp),
        out_shape=(
            jax.ShapeDtypeStruct((three, n_tp, ff_here // n_sp, depth * n_sp), weights.dtype),
            jax.ShapeDtypeStruct((kv.shape[0] * n_sp, kv.shape[1]), kv.dtype),
        ),
        in_specs=[pl.BlockSpec(memory_space=pltpu.VMEM)] * 2,
        out_specs=[pl.BlockSpec(memory_space=pltpu.VMEM)] * 2,
        scratch_shapes=[dma((n_sp - 1,))] * 4 + [dma((n_sp,))] * 6 + [dma((2,))],
        compiler_params=pltpu.CompilerParams(
            collective_id=0, has_side_effects=True, vmem_limit_bytes=48 * 2**20
        ),
        name="spread",
    )(weights, kv)


def middle_kernel(
    n_sp, n_tp, part_ref, res_ref, gain_ref, resid_ref, nall, pbuf, rbuf, nbuf,
    p_s, p_r, q_s, q_r, z_s, z_r, y_s, y_r,
):
    s, t, y_peer, _, _ = neighbours(n_sp, n_tp)
    half = n_sp // 2
    rows = nbuf.shape[0]
    cols = res_ref.shape[1]
    greet(
        [{"tp": lax.rem(t + j, n_tp)} for j in range(1, n_tp)]
        + [{"sp": y_peer}]
        + [{"sp": lax.rem(s + 2 * j, n_sp)} for j in range(1, half)]
    )
    sent = []

    def take(p):
        return pl.ds(pl.multiple_of(p * rows, rows), rows)

    here = pl.ds(pl.multiple_of(t * cols, cols), cols)
    for j in range(1, n_tp):
        p = lax.rem(t + j, n_tp)
        one = remote(part_ref.at[take(p), :], pbuf.at[j - 1], p_s.at[j - 1], p_r.at[j - 1], {"tp": p})
        two = remote(
            res_ref.at[take(p), :], rbuf.at[:, here], q_s.at[j - 1], q_r.at[j - 1], {"tp": p}
        )
        one.start()
        two.start()
        sent += [one, two]
    rbuf[:, here] = res_ref[take(t), :]
    total = part_ref[take(t), :].astype(jnp.float32)
    for copy in sent:
        copy.wait()
    for j in range(1, n_tp):
        total = total + pbuf[j - 1].astype(jnp.float32)
    resid = (rbuf[...].astype(jnp.float32) + total).astype(jnp.bfloat16)
    resid_ref[...] = resid
    wide = resid.astype(jnp.float32)
    mean = jnp.mean(wide * wide, axis=1, keepdims=True)
    normed = (wide * lax.rsqrt(mean + epsilon) * gain_ref[...]).astype(jnp.bfloat16)
    nbuf[...] = normed
    z_in, y_in = [], []
    for j in range(1, half):
        copy = remote(
            nbuf, nall.at[s], z_s.at[j - 1], z_r.at[j - 1], {"sp": lax.rem(s + 2 * j, n_sp)}
        )
        copy.start()
        z_in.append(copy)
    copy = remote(nbuf, nall.at[s], y_s.at[0], y_r.at[0], {"sp": y_peer})
    copy.start()
    y_in.append(copy)
    nall[s] = normed
    for j in range(1, half):
        z_in[j - 1].wait_recv()
        source = lax.rem(s - 2 * j + n_sp, n_sp)
        copy = remote(nall.at[source], nall.at[source], y_s.at[j], y_r.at[j], {"sp": y_peer})
        copy.start()
        y_in.append(copy)
    for copy in z_in:
        copy.wait_send()
    for copy in y_in:
        copy.wait()


def middle(part, residual, gain, n_sp, n_tp):
    rows, width = part.shape[0] // n_tp, part.shape[1]
    dma = pltpu.SemaphoreType.DMA
    half = n_sp // 2
    return pl.pallas_call(
        functools.partial(middle_kernel, n_sp, n_tp),
        out_shape=(
            jax.ShapeDtypeStruct((rows, width), jnp.bfloat16),
            jax.ShapeDtypeStruct((n_sp, rows, width), jnp.bfloat16),
        ),
        in_specs=[pl.BlockSpec(memory_space=pltpu.VMEM)] * 3,
        out_specs=[pl.BlockSpec(memory_space=pltpu.VMEM)] * 2,
        scratch_shapes=[
            pltpu.VMEM((n_tp - 1, rows, width), jnp.bfloat16),
            pltpu.VMEM((rows, width), jnp.bfloat16),
            pltpu.VMEM((rows, width), jnp.bfloat16),
        ]
        + [dma((n_tp - 1,))] * 4
        + [dma((half - 1,))] * 2
        + [dma((half,))] * 2,
        compiler_params=pltpu.CompilerParams(collective_id=1, has_side_effects=True),
        name="middle",
    )(part, residual, gain)


def finish_kernel(
    n_sp, n_tp, part_ref, resid_ref, out_ref, ybuf, cbuf, zbuf, fbuf,
    y_s, y_r, z_s, z_r, o_s, o_r,
):
    s, t, y_peer, _, _ = neighbours(n_sp, n_tp)
    half = n_sp // 2
    rows = fbuf.shape[0]
    cols = out_ref.shape[1]
    greet(
        [{"tp": lax.rem(t + j, n_tp)} for j in range(1, n_tp)]
        + [{"sp": y_peer}]
        + [{"sp": lax.rem(s + 2 * j, n_sp)} for j in range(1, half)]
    )
    order = list(range(1, half)) + [0]
    y_in = {}
    for j in order:
        copy = remote(
            part_ref.at[lax.rem(y_peer + 2 * j, n_sp)], ybuf.at[j], y_s.at[j], y_r.at[j],
            {"sp": y_peer},
        )
        copy.start()
        y_in[j] = copy
    z_in = []
    for j in order:
        y_in[j].wait_recv()
        both = part_ref[lax.rem(s + 2 * j, n_sp)].astype(jnp.float32) + ybuf[j].astype(jnp.float32)
        if j == 0:
            total = both
        else:
            cbuf[j - 1] = both.astype(jnp.bfloat16)
            copy = remote(
                cbuf.at[j - 1], zbuf.at[j - 1], z_s.at[j - 1], z_r.at[j - 1],
                {"sp": lax.rem(s + 2 * j, n_sp)},
            )
            copy.start()
            z_in.append(copy)
    for j in range(1, half):
        z_in[j - 1].wait_recv()
        total = total + zbuf[j - 1].astype(jnp.float32)
    fbuf[...] = (resid_ref[...].astype(jnp.float32) + total).astype(jnp.bfloat16)
    mine = pl.ds(pl.multiple_of(t * rows, rows), rows)
    out = []
    for j in range(1, n_tp):
        p = lax.rem(t + j, n_tp)
        copy = remote(
            fbuf.at[:, pl.ds(pl.multiple_of(p * cols, cols), cols)], out_ref.at[mine, :],
            o_s.at[j - 1], o_r.at[j - 1], {"tp": p},
        )
        copy.start()
        out.append(copy)
    out_ref[mine, :] = fbuf[:, pl.ds(pl.multiple_of(t * cols, cols), cols)]
    for copy in out:
        copy.wait()
    for j in order:
        y_in[j].wait_send()
    for copy in z_in:
        copy.wait_send()


def finish(part, resid, n_sp, n_tp):
    _, rows, width = part.shape
    dma = pltpu.SemaphoreType.DMA
    half = n_sp // 2
    block = (rows, width)
    return pl.pallas_call(
        functools.partial(finish_kernel, n_sp, n_tp),
        out_shape=jax.ShapeDtypeStruct((rows * n_tp, width // n_tp), jnp.bfloat16),
        in_specs=[pl.BlockSpec(memory_space=pltpu.VMEM)] * 2,
        out_specs=pl.BlockSpec(memory_space=pltpu.VMEM),
        scratch_shapes=[
            pltpu.VMEM((half,) + block, jnp.bfloat16),
            pltpu.VMEM((half - 1,) + block, jnp.bfloat16),
            pltpu.VMEM((half - 1,) + block, jnp.bfloat16),
            pltpu.VMEM(block, jnp.bfloat16),
        ]
        + [dma((half,))] * 2
        + [dma((half - 1,))] * 2
        + [dma((n_tp - 1,))] * 2,
        compiler_params=pltpu.CompilerParams(collective_id=2, has_side_effects=True),
        name="finish",
    )(part, resid)


def last_dot(left, right):
    return lax.dot_general(
        left, right, (((1,), (1,)), ((), ())), preferred_element_type=jnp.float32
    )


def split_hidden(
    n_sp,
    n_tp,
    queries_one,
    queries_two,
    keys_one,
    keys_two,
    values,
    mix_lambda,
    head_gain,
    out_weight,
    residual_in,
    norm_gain,
    gate_weight,
    up_weight,
    down_weight,
):
    tok_rows = queries_one.shape[0]
    weights = jnp.stack([gate_weight.T, up_weight.T, down_weight])
    kv = jnp.concatenate([keys_one, keys_two, values], axis=1)
    wall, kvall = spread(weights, kv, n_sp, n_tp)
    query_pos = lax.axis_index("sp") * tok_rows + jnp.arange(tok_rows, dtype=jnp.int32)
    key_pos = jnp.arange(kvall.shape[0], dtype=jnp.int32)
    visible = key_pos[None, :] <= query_pos[:, None]
    value_rows = kvall[:, 2 * HEAD :]

    def one_map(queries, key_rows):
        scores = last_dot(queries, key_rows) * HEAD ** (-0.5)
        scores = jnp.where(visible, scores, masked_score)
        weights_exp = jnp.exp(scores - jnp.max(scores, axis=1, keepdims=True))
        totals = jnp.sum(weights_exp, axis=1, keepdims=True)
        return (
            jnp.dot(
                weights_exp.astype(jnp.bfloat16), value_rows, preferred_element_type=jnp.float32
            )
            / totals
        )

    mixed = one_map(queries_one, kvall[:, :HEAD]) - mix_lambda[0] * one_map(
        queries_two, kvall[:, HEAD : 2 * HEAD]
    )
    mean_square = jnp.mean(mixed * mixed, axis=1, keepdims=True)
    attended = (mixed * lax.rsqrt(mean_square + epsilon) * head_gain[None, :] * 0.8).astype(
        jnp.bfloat16
    )
    projected = jnp.dot(attended, out_weight, preferred_element_type=jnp.float32).astype(
        jnp.bfloat16
    )
    resid, nall = middle(projected, residual_in, norm_gain[None, :], n_sp, n_tp)
    width = nall.shape[2]
    normed = nall.reshape(-1, width)
    stacked = wall.reshape(3, -1, width)
    gate_act = last_dot(normed, stacked[0])
    up_act = last_dot(normed, stacked[1])
    hidden = (jax.nn.silu(gate_act) * up_act).astype(jnp.bfloat16)
    partials = jnp.dot(hidden, stacked[2], preferred_element_type=jnp.float32).astype(jnp.bfloat16)
    return finish(partials.reshape(nall.shape), resid, n_sp, n_tp)


def fits(n_sp, n_tp, shapes):
    tokens, ff, width, heads = shapes
    part = ff // (n_sp * n_tp)
    return (
        n_tp == 4
        and heads == n_tp
        and n_sp % 2 == 0
        and n_sp > 2
        and part % 16 == 0
        and width % (n_sp * 128) == 0
        and tokens % (n_sp * n_tp * 16) == 0
        and tokens * width <= 2**23
    )


def solution(mesh):
    in_specs = (
        P("sp", "tp"),
        P("sp", "tp"),
        P("sp", "tp"),
        P("sp", "tp"),
        P("sp", "tp"),
        P("tp"),
        P("tp"),
        P("tp", None),
        P("sp", "tp"),
        P(),
        P("sp", "tp"),
        P("sp", "tp"),
        P("tp", "sp"),
    )
    out_specs = P("sp", "tp")
    n_sp, n_tp = mesh.shape["sp"], mesh.shape["tp"]

    def layer(*args):
        shapes = (args[0].shape[0], args[10].shape[1], args[10].shape[0], args[5].shape[0])
        body = per_device
        if fits(n_sp, n_tp, shapes):
            body = functools.partial(split_hidden, n_sp, n_tp)
        return jax.shard_map(
            body, mesh=mesh, in_specs=in_specs, out_specs=out_specs, check_vma=False
        )(*args)

    return layer
```

```python
import functools

import jax
import jax.numpy as jnp
from jax import lax
from jax.experimental import pallas as pl
from jax.experimental.pallas import tpu as pltpu
from jax.sharding import PartitionSpec as P

HEAD = 128


epsilon = 1e-06
masked_score = -1e30


def per_device(
    queries_one,
    queries_two,
    keys_one,
    keys_two,
    values,
    mix_lambda,
    head_gain,
    out_weight,
    residual_in,
    norm_gain,
    gate_weight,
    up_weight,
    down_weight,
):
    tok_rows = queries_one.shape[0]
    heads_here = mix_lambda.shape[0]
    head_width = HEAD
    value_width = values.shape[1] // heads_here
    query_pos = lax.axis_index("sp") * tok_rows + jnp.arange(tok_rows, dtype=jnp.int32)
    query_first = queries_one.reshape(tok_rows, heads_here, head_width)
    query_second = queries_two.reshape(tok_rows, heads_here, head_width)
    score_scale = head_width ** (-0.5)

    def update(state, queries, key_rows, value_rows, visible):
        running, totals, weighted = state
        scores = (
            jnp.einsum("qhd,khd->hqk", queries, key_rows, preferred_element_type=jnp.float32)
            * score_scale
        )
        scores = jnp.where(visible[None], scores, masked_score)
        highest = jnp.maximum(running, jnp.max(scores, axis=2))
        weights_exp = jnp.where(visible[None], jnp.exp(scores - highest[..., None]), 0.0)
        totals = jnp.sum(weights_exp, axis=2)
        weighted = jnp.einsum(
            "hqk,khd->hqd",
            weights_exp.astype(jnp.bfloat16),
            value_rows,
            preferred_element_type=jnp.float32,
        )
        return (highest, totals, weighted)

    initial = (
        jnp.full((heads_here, tok_rows), masked_score, jnp.float32),
        jnp.zeros((heads_here, tok_rows), jnp.float32),
        jnp.zeros((heads_here, tok_rows, value_width), jnp.float32),
    )
    key_first = lax.all_gather(keys_one, "sp", axis=0, tiled=True)
    key_second = lax.all_gather(keys_two, "sp", axis=0, tiled=True)
    value_piece = lax.all_gather(values, "sp", axis=0, tiled=True)
    key_count = key_first.shape[0]
    key_pos = jnp.arange(key_count, dtype=jnp.int32)
    visible = key_pos[None, :] <= query_pos[:, None]
    value_rows = value_piece.reshape(key_count, heads_here, value_width)
    first_new = update(
        initial,
        query_first,
        key_first.reshape(key_count, heads_here, head_width),
        value_rows,
        visible,
    )
    second_new = update(
        initial,
        query_second,
        key_second.reshape(key_count, heads_here, head_width),
        value_rows,
        visible,
    )
    lam_heads = mix_lambda[:, None, None]
    mixed = (
        first_new[2] / first_new[1][..., None]
        - lam_heads * second_new[2] / second_new[1][..., None]
    )
    mean_square = jnp.mean(mixed * mixed, axis=2, keepdims=True)
    normed_heads = (
        mixed
        * lax.rsqrt(mean_square + epsilon)
        * head_gain.reshape(heads_here, 1, value_width)
        * 0.8
    )
    attended = (
        normed_heads.transpose(1, 0, 2)
        .reshape(tok_rows, heads_here * value_width)
        .astype(jnp.bfloat16)
    )
    projected = lax.psum_scatter(
        lax.dot_general(
            out_weight, attended, (((0,), (1,)), ((), ())), preferred_element_type=jnp.float32
        ).astype(jnp.bfloat16),
        "tp",
        scatter_dimension=0,
        tiled=True,
    ).astype(jnp.float32)
    resid = (residual_in.astype(jnp.float32) + projected.T).astype(jnp.bfloat16)
    full_rows = lax.all_gather(resid, "tp", axis=1, tiled=True)
    full_float = full_rows.astype(jnp.float32)
    mean_rows = jnp.mean(full_float * full_float, axis=1, keepdims=True)
    normed = (full_float * lax.rsqrt(mean_rows + epsilon) * norm_gain[None, :]).astype(jnp.bfloat16)
    gate_act = jnp.dot(
        normed,
        lax.all_gather(gate_weight, "sp", axis=0, tiled=True),
        preferred_element_type=jnp.float32,
    )
    up_act = jnp.dot(
        normed,
        lax.all_gather(up_weight, "sp", axis=0, tiled=True),
        preferred_element_type=jnp.float32,
    )
    hidden = (jax.nn.silu(gate_act) * up_act).astype(jnp.bfloat16)
    partials = jnp.dot(
        hidden,
        lax.all_gather(down_weight, "sp", axis=1, tiled=True),
        preferred_element_type=jnp.float32,
    )
    mlp_out = lax.psum_scatter(
        partials.astype(jnp.bfloat16), "tp", scatter_dimension=1, tiled=True
    ).astype(jnp.float32)
    return (resid.astype(jnp.float32) + mlp_out).astype(jnp.bfloat16)


def remote(src, dst, send, recv, where):
    return pltpu.make_async_remote_copy(
        src_ref=src,
        dst_ref=dst,
        send_sem=send,
        recv_sem=recv,
        device_id=where,
        device_id_type=pl.DeviceIdType.MESH,
    )


def greet(peers):
    barrier = pltpu.get_barrier_semaphore()
    for where in peers:
        pl.semaphore_signal(
            barrier, inc=1, device_id=where, device_id_type=pl.DeviceIdType.MESH
        )
    pl.semaphore_wait(barrier, len(peers))


def neighbours(n_sp, n_tp):
    s, t = lax.axis_index("sp"), lax.axis_index("tp")
    y_peer = s + 1 - 2 * lax.rem(s, 2)
    sibling = t + 1 - 2 * lax.rem(t, 2)
    across = lax.rem(t + 2, n_tp)
    return s, t, y_peer, sibling, across


def front_kernel(
    n_sp, n_tp, w_ref, kv_ref, q1_ref, q2_ref, lam_ref, hgain_ref, ow_ref, res_ref, gain_ref,
    wall, resid_ref, nall,
    kvall, top, low, acc, part_ref, pbuf, rbuf, nbuf, *sems,
):
    (h_s, h_r, v_s, v_r, a_s, a_r, x_s, x_r, c_s, c_r, f_s, f_r, loc,
     p_s, p_r, r_s, r_r, z_s, z_r, y_s, y_r) = sems
    s, t, y_peer, sibling, across = neighbours(n_sp, n_tp)
    z = lax.div(s, 2)
    half = n_sp // 2
    rows = kv_ref.shape[0]
    part = w_ref.shape[1] // n_sp
    depth = w_ref.shape[2]
    greet(
        [{"sp": lax.rem(s + i, n_sp)} for i in range(1, n_sp)]
        + [{"tp": lax.rem(t + j, n_tp)} for j in range(1, n_tp)]
    )

    def block(who, source):
        return wall.at[:, who, :, pl.ds(pl.multiple_of(source * depth, depth), depth)]

    def piece(dest):
        return w_ref.at[:, pl.ds(pl.multiple_of(dest * part, 16), part), :]

    def weight(i):
        p = lax.rem(s + i, n_sp)
        return remote(piece(p), block(t, s), a_s.at[i - 1], a_r.at[i - 1], {"sp": p})

    def kv_rows(who):
        return kvall.at[pl.ds(pl.multiple_of(who * rows, rows), rows), :]

    def hop(j):
        who = s - 2 * j
        src = kv_ref if j == 0 else kv_rows(who)
        return remote(src, kv_rows(who), h_s.at[j], h_r.at[j], {"sp": lax.rem(s + 2, n_sp)})

    def hop_in(j):
        who = kv_rows(s - 2 - 2 * j)
        return remote(who, who, h_s.at[j], h_r.at[j], {"sp": lax.rem(s + 2, n_sp)})

    def over(j):
        who = s - 2 * j
        src = kv_ref if j == 0 else kv_rows(who)
        return remote(src, kv_rows(who), v_s.at[j], v_r.at[j], {"sp": y_peer})

    def over_in(j):
        who = kv_rows(y_peer - 2 * j)
        return remote(who, who, v_s.at[j], v_r.at[j], {"sp": y_peer})

    own_kv = pltpu.make_async_copy(kv_ref, kv_rows(s), loc.at[0])
    own_kv.start()
    own_w = pltpu.make_async_copy(piece(s), block(t, s), loc.at[1])
    own_w.start()

    @pl.when(z < half - 1)
    def _():
        hop(0).start()

    over(0).start()
    even = list(range(2, n_sp, 2))
    odd = list(range(1, n_sp, 2))
    for i in even:

        @pl.when(s + i >= n_sp)
        def _(i=i):
            weight(i).start()

    for j in range(1, half):

        @pl.when(z >= j)
        def _(j=j):
            hop_in(j - 1).wait_recv()
            if j < half - 1:

                @pl.when(z < half - 1)
                def _():
                    hop(j).start()

            over(j).start()

    for i in even:

        @pl.when(s + i < n_sp)
        def _(i=i):
            weight(i).start()

    for i in odd:
        weight(i).start()

    def across_copy(i):
        source = lax.rem(s - i + n_sp, n_sp)
        return remote(
            block(t, source), block(t, source), x_s.at[i], x_r.at[i], {"tp": across}
        )

    def sibling_copy(i):
        source = lax.rem(s - i + n_sp, n_sp)
        return remote(
            block(t, source), block(t, source), c_s.at[i], c_r.at[i], {"tp": sibling}
        )

    def second_copy(i):
        source = lax.rem(s - i + n_sp, n_sp)
        return remote(
            block(across, source), block(across, source), f_s.at[i], f_r.at[i], {"tp": sibling}
        )

    def relay(i):
        if i == 0:
            own_w.wait()
        else:
            weight(i).wait_recv()
        across_copy(i).start()
        sibling_copy(i).start()

    def second(i):
        across_copy(i).wait_recv()
        second_copy(i).start()

    query_refs = (q1_ref, q2_ref)

    def attend(j):
        first = (z - j) * (2 * rows)
        keys = pl.ds(pl.multiple_of(first, 2 * rows), 2 * rows)
        for c in range(2):
            scores = last_dot(
                query_refs[c][...], kvall[keys, c * HEAD : (c + 1) * HEAD]
            ) * HEAD ** (-0.5)
            if j == 0:
                query_pos = s * rows + lax.broadcasted_iota(jnp.int32, scores.shape, 0)
                key_pos = first + lax.broadcasted_iota(jnp.int32, scores.shape, 1)
                scores = jnp.where(key_pos <= query_pos, scores, masked_score)
            highest = jnp.max(scores, axis=1, keepdims=True)
            if j > 0:
                highest = jnp.maximum(highest, top[c])
            weights_exp = jnp.exp(scores - highest)
            total = jnp.sum(weights_exp, axis=1, keepdims=True)
            weighted = jnp.dot(
                weights_exp.astype(jnp.bfloat16),
                kvall[keys, 2 * HEAD :],
                preferred_element_type=jnp.float32,
            )
            if j > 0:
                keep = jnp.exp(top[c] - highest)
                total = total + keep * low[c]
                weighted = weighted + keep * acc[c]
            top[c] = highest
            low[c] = total
            acc[c] = weighted

    order = [0] + even + odd
    own_kv.wait()
    relay(order[0])
    over_in(0).wait_recv()
    attend(0)
    done, crossed = 1, 0
    for j in range(1, half):
        relay(order[done])
        done += 1

        @pl.when(z >= j)
        def _(j=j):
            over_in(j).wait_recv()
            attend(j)

        second(order[crossed])
        crossed += 1

    mixed = acc[0] / low[0] - lam_ref[0, 0] * acc[1] / low[1]
    mean_square = jnp.mean(mixed * mixed, axis=1, keepdims=True)
    attended = (mixed * lax.rsqrt(mean_square + epsilon) * hgain_ref[...] * 0.8).astype(
        jnp.bfloat16
    )
    width = ow_ref.shape[1]
    for k in range(0, width, 512):
        part_ref[:, k : k + 512] = jnp.dot(
            attended, ow_ref[:, k : k + 512], preferred_element_type=jnp.float32
        ).astype(jnp.bfloat16)

    out_rows = nbuf.shape[0]
    cols = res_ref.shape[1]
    sent = []

    def take(p):
        return pl.ds(pl.multiple_of(p * out_rows, out_rows), out_rows)

    here = pl.ds(pl.multiple_of(t * cols, cols), cols)
    for j in range(1, n_tp):
        p = lax.rem(t + j, n_tp)
        one = remote(part_ref.at[take(p), :], pbuf.at[j - 1], p_s.at[j - 1], p_r.at[j - 1], {"tp": p})
        two = remote(
            res_ref.at[take(p), :], rbuf.at[:, here], r_s.at[j - 1], r_r.at[j - 1], {"tp": p}
        )
        one.start()
        two.start()
        sent += [one, two]
    rbuf[:, here] = res_ref[take(t), :]
    while done < n_sp:
        relay(order[done])
        done += 1
        second(order[crossed])
        crossed += 1
    total = part_ref[take(t), :].astype(jnp.float32)
    for copy in sent:
        copy.wait()
    for j in range(1, n_tp):
        total = total + pbuf[j - 1].astype(jnp.float32)
    resid = (rbuf[...].astype(jnp.float32) + total).astype(jnp.bfloat16)
    resid_ref[...] = resid
    wide = resid.astype(jnp.float32)
    mean = jnp.mean(wide * wide, axis=1, keepdims=True)
    normed = (wide * lax.rsqrt(mean + epsilon) * gain_ref[...]).astype(jnp.bfloat16)
    nbuf[...] = normed
    z_in, y_in = [], []
    copy = remote(nbuf, nall.at[s], y_s.at[0], y_r.at[0], {"sp": y_peer})
    copy.start()
    y_in.append(copy)
    for j in range(1, half):
        copy = remote(
            nbuf, nall.at[s], z_s.at[j - 1], z_r.at[j - 1], {"sp": lax.rem(s + 2 * j, n_sp)}
        )
        copy.start()
        z_in.append(copy)
    nall[s] = normed
    while crossed < n_sp:
        second(order[crossed])
        crossed += 1
    for j in range(1, half):
        z_in[j - 1].wait_recv()
        source = lax.rem(s - 2 * j + n_sp, n_sp)
        copy = remote(nall.at[source], nall.at[source], y_s.at[j], y_r.at[j], {"sp": y_peer})
        copy.start()
        y_in.append(copy)
    for copy in z_in:
        copy.wait_send()
    for copy in y_in:
        copy.wait()
    for i in range(n_sp):
        if i > 0:
            weight(i).wait_send()
        across_copy(i).wait_send()
        sibling_copy(i).wait_send()
        second_copy(i).wait_send()
        source = lax.rem(s - i + n_sp, n_sp)
        theirs = block(sibling, source)
        remote(theirs, theirs, c_s.at[i], c_r.at[i], {"tp": sibling}).wait_recv()
        theirs = block(lax.rem(sibling + 2, n_tp), source)
        remote(theirs, theirs, f_s.at[i], f_r.at[i], {"tp": sibling}).wait_recv()
    over(0).wait_send()

    @pl.when(z < half - 1)
    def _():
        hop(0).wait_send()

    for j in range(1, half):

        @pl.when(z >= j)
        def _(j=j):
            over(j).wait_send()
            if j < half - 1:

                @pl.when(z < half - 1)
                def _():
                    hop(j).wait_send()


def front(weights, kv, q1, q2, lam, hgain, ow, res, gain, n_sp, n_tp):
    three, ff_here, depth = weights.shape
    tok, width = kv.shape[0], ow.shape[1]
    rows = tok // n_tp
    half = n_sp // 2
    dma = pltpu.SemaphoreType.DMA
    vmem = pl.BlockSpec(memory_space=pltpu.VMEM)
    bf16, f32 = jnp.bfloat16, jnp.float32
    return pl.pallas_call(
        functools.partial(front_kernel, n_sp, n_tp),
        out_shape=(
            jax.ShapeDtypeStruct((three, n_tp, ff_here // n_sp, depth * n_sp), bf16),
            jax.ShapeDtypeStruct((rows, width), bf16),
            jax.ShapeDtypeStruct((n_sp, rows, width), bf16),
        ),
        in_specs=[vmem] * 4 + [pl.BlockSpec(memory_space=pltpu.SMEM)] + [vmem] * 4,
        out_specs=[vmem] * 3,
        scratch_shapes=[
            pltpu.VMEM((tok * n_sp, kv.shape[1]), bf16),
            pltpu.VMEM((2, tok, 1), f32),
            pltpu.VMEM((2, tok, 1), f32),
            pltpu.VMEM((2, tok, ow.shape[0]), f32),
            pltpu.VMEM((tok, width), bf16),
            pltpu.VMEM((n_tp - 1, rows, width), bf16),
            pltpu.VMEM((rows, width), bf16),
            pltpu.VMEM((rows, width), bf16),
        ]
        + [dma((half,))] * 4
        + [dma((n_sp - 1,))] * 2
        + [dma((n_sp,))] * 6
        + [dma((2,))]
        + [dma((n_tp - 1,))] * 4
        + [dma((half - 1,))] * 2
        + [dma((half,))] * 2,
        compiler_params=pltpu.CompilerParams(
            collective_id=0, has_side_effects=True, vmem_limit_bytes=48 * 2**20
        ),
        name="front",
    )(weights, kv, q1, q2, lam, hgain, ow, res, gain)


def finish_kernel(
    n_sp, n_tp, part_ref, resid_ref, out_ref, ybuf, cbuf, zbuf, fbuf,
    y_s, y_r, z_s, z_r, o_s, o_r,
):
    s, t, y_peer, _, _ = neighbours(n_sp, n_tp)
    half = n_sp // 2
    rows = fbuf.shape[0]
    cols = out_ref.shape[1]
    greet(
        [{"tp": lax.rem(t + j, n_tp)} for j in range(1, n_tp)]
        + [{"sp": y_peer}]
        + [{"sp": lax.rem(s + 2 * j, n_sp)} for j in range(1, half)]
    )
    order = list(range(1, half)) + [0]
    y_in = {}
    for j in order:
        copy = remote(
            part_ref.at[lax.rem(y_peer + 2 * j, n_sp)], ybuf.at[j], y_s.at[j], y_r.at[j],
            {"sp": y_peer},
        )
        copy.start()
        y_in[j] = copy
    z_in = []
    for j in order:
        y_in[j].wait_recv()
        both = part_ref[lax.rem(s + 2 * j, n_sp)].astype(jnp.float32) + ybuf[j].astype(jnp.float32)
        if j == 0:
            total = both
        else:
            cbuf[j - 1] = both.astype(jnp.bfloat16)
            copy = remote(
                cbuf.at[j - 1], zbuf.at[j - 1], z_s.at[j - 1], z_r.at[j - 1],
                {"sp": lax.rem(s + 2 * j, n_sp)},
            )
            copy.start()
            z_in.append(copy)
    for j in range(1, half):
        z_in[j - 1].wait_recv()
        total = total + zbuf[j - 1].astype(jnp.float32)
    fbuf[...] = (resid_ref[...].astype(jnp.float32) + total).astype(jnp.bfloat16)
    mine = pl.ds(pl.multiple_of(t * rows, rows), rows)
    out = []
    for j in range(1, n_tp):
        p = lax.rem(t + j, n_tp)
        copy = remote(
            fbuf.at[:, pl.ds(pl.multiple_of(p * cols, cols), cols)], out_ref.at[mine, :],
            o_s.at[j - 1], o_r.at[j - 1], {"tp": p},
        )
        copy.start()
        out.append(copy)
    out_ref[mine, :] = fbuf[:, pl.ds(pl.multiple_of(t * cols, cols), cols)]
    for copy in out:
        copy.wait()
    for j in order:
        y_in[j].wait_send()
    for copy in z_in:
        copy.wait_send()


def finish(part, resid, n_sp, n_tp):
    _, rows, width = part.shape
    dma = pltpu.SemaphoreType.DMA
    half = n_sp // 2
    block = (rows, width)
    return pl.pallas_call(
        functools.partial(finish_kernel, n_sp, n_tp),
        out_shape=jax.ShapeDtypeStruct((rows * n_tp, width // n_tp), jnp.bfloat16),
        in_specs=[pl.BlockSpec(memory_space=pltpu.VMEM)] * 2,
        out_specs=pl.BlockSpec(memory_space=pltpu.VMEM),
        scratch_shapes=[
            pltpu.VMEM((half,) + block, jnp.bfloat16),
            pltpu.VMEM((half - 1,) + block, jnp.bfloat16),
            pltpu.VMEM((half - 1,) + block, jnp.bfloat16),
            pltpu.VMEM(block, jnp.bfloat16),
        ]
        + [dma((half,))] * 2
        + [dma((half - 1,))] * 2
        + [dma((n_tp - 1,))] * 2,
        compiler_params=pltpu.CompilerParams(collective_id=2, has_side_effects=True),
        name="finish",
    )(part, resid)


def last_dot(left, right):
    return lax.dot_general(
        left, right, (((1,), (1,)), ((), ())), preferred_element_type=jnp.float32
    )


def split_hidden(
    n_sp,
    n_tp,
    queries_one,
    queries_two,
    keys_one,
    keys_two,
    values,
    mix_lambda,
    head_gain,
    out_weight,
    residual_in,
    norm_gain,
    gate_weight,
    up_weight,
    down_weight,
):
    weights = jnp.stack([gate_weight.T, up_weight.T, down_weight])
    kv = jnp.concatenate([keys_one, keys_two, values], axis=1)
    wall, resid, nall = front(
        weights,
        kv,
        queries_one,
        queries_two,
        mix_lambda[None, :],
        head_gain[None, :],
        out_weight,
        residual_in,
        norm_gain[None, :],
        n_sp,
        n_tp,
    )
    width = nall.shape[2]
    normed = nall.reshape(-1, width)
    stacked = wall.reshape(3, -1, width)
    gate_act = last_dot(normed, stacked[0])
    up_act = last_dot(normed, stacked[1])
    hidden = (jax.nn.silu(gate_act) * up_act).astype(jnp.bfloat16)
    partials = jnp.dot(hidden, stacked[2], preferred_element_type=jnp.float32).astype(jnp.bfloat16)
    return finish(partials.reshape(nall.shape), resid, n_sp, n_tp)


def fits(n_sp, n_tp, shapes):
    tokens, ff, width, heads = shapes
    part = ff // (n_sp * n_tp)
    return (
        n_tp == 4
        and heads == n_tp
        and n_sp % 2 == 0
        and n_sp > 2
        and part % 16 == 0
        and width % (n_sp * 128) == 0
        and tokens % (n_sp * n_tp * 16) == 0
        and tokens * width <= 2**23
    )


def solution(mesh):
    in_specs = (
        P("sp", "tp"),
        P("sp", "tp"),
        P("sp", "tp"),
        P("sp", "tp"),
        P("sp", "tp"),
        P("tp"),
        P("tp"),
        P("tp", None),
        P("sp", "tp"),
        P(),
        P("sp", "tp"),
        P("sp", "tp"),
        P("tp", "sp"),
    )
    out_specs = P("sp", "tp")
    n_sp, n_tp = mesh.shape["sp"], mesh.shape["tp"]

    def layer(*args):
        shapes = (args[0].shape[0], args[10].shape[1], args[10].shape[0], args[5].shape[0])
        body = per_device
        if fits(n_sp, n_tp, shapes):
            body = functools.partial(split_hidden, n_sp, n_tp)
        return jax.shard_map(
            body, mesh=mesh, in_specs=in_specs, out_specs=out_specs, check_vma=False
        )(*args)

    return layer
```

```python
import functools

import jax
import jax.numpy as jnp
from jax import lax
from jax.experimental import pallas as pl
from jax.experimental.pallas import tpu as pltpu
from jax.sharding import PartitionSpec as P

HEAD = 128


epsilon = 1e-06
masked_score = -1e30


def per_device(
    queries_one,
    queries_two,
    keys_one,
    keys_two,
    values,
    mix_lambda,
    head_gain,
    out_weight,
    residual_in,
    norm_gain,
    gate_weight,
    up_weight,
    down_weight,
):
    tok_rows = queries_one.shape[0]
    heads_here = mix_lambda.shape[0]
    head_width = HEAD
    value_width = values.shape[1] // heads_here
    query_pos = lax.axis_index("sp") * tok_rows + jnp.arange(tok_rows, dtype=jnp.int32)
    query_first = queries_one.reshape(tok_rows, heads_here, head_width)
    query_second = queries_two.reshape(tok_rows, heads_here, head_width)
    score_scale = head_width ** (-0.5)

    def update(state, queries, key_rows, value_rows, visible):
        running, totals, weighted = state
        scores = (
            jnp.einsum("qhd,khd->hqk", queries, key_rows, preferred_element_type=jnp.float32)
            * score_scale
        )
        scores = jnp.where(visible[None], scores, masked_score)
        highest = jnp.maximum(running, jnp.max(scores, axis=2))
        weights_exp = jnp.where(visible[None], jnp.exp(scores - highest[..., None]), 0.0)
        totals = jnp.sum(weights_exp, axis=2)
        weighted = jnp.einsum(
            "hqk,khd->hqd",
            weights_exp.astype(jnp.bfloat16),
            value_rows,
            preferred_element_type=jnp.float32,
        )
        return (highest, totals, weighted)

    initial = (
        jnp.full((heads_here, tok_rows), masked_score, jnp.float32),
        jnp.zeros((heads_here, tok_rows), jnp.float32),
        jnp.zeros((heads_here, tok_rows, value_width), jnp.float32),
    )
    key_first = lax.all_gather(keys_one, "sp", axis=0, tiled=True)
    key_second = lax.all_gather(keys_two, "sp", axis=0, tiled=True)
    value_piece = lax.all_gather(values, "sp", axis=0, tiled=True)
    key_count = key_first.shape[0]
    key_pos = jnp.arange(key_count, dtype=jnp.int32)
    visible = key_pos[None, :] <= query_pos[:, None]
    value_rows = value_piece.reshape(key_count, heads_here, value_width)
    first_new = update(
        initial,
        query_first,
        key_first.reshape(key_count, heads_here, head_width),
        value_rows,
        visible,
    )
    second_new = update(
        initial,
        query_second,
        key_second.reshape(key_count, heads_here, head_width),
        value_rows,
        visible,
    )
    lam_heads = mix_lambda[:, None, None]
    mixed = (
        first_new[2] / first_new[1][..., None]
        - lam_heads * second_new[2] / second_new[1][..., None]
    )
    mean_square = jnp.mean(mixed * mixed, axis=2, keepdims=True)
    normed_heads = (
        mixed
        * lax.rsqrt(mean_square + epsilon)
        * head_gain.reshape(heads_here, 1, value_width)
        * 0.8
    )
    attended = (
        normed_heads.transpose(1, 0, 2)
        .reshape(tok_rows, heads_here * value_width)
        .astype(jnp.bfloat16)
    )
    projected = lax.psum_scatter(
        lax.dot_general(
            out_weight, attended, (((0,), (1,)), ((), ())), preferred_element_type=jnp.float32
        ).astype(jnp.bfloat16),
        "tp",
        scatter_dimension=0,
        tiled=True,
    ).astype(jnp.float32)
    resid = (residual_in.astype(jnp.float32) + projected.T).astype(jnp.bfloat16)
    full_rows = lax.all_gather(resid, "tp", axis=1, tiled=True)
    full_float = full_rows.astype(jnp.float32)
    mean_rows = jnp.mean(full_float * full_float, axis=1, keepdims=True)
    normed = (full_float * lax.rsqrt(mean_rows + epsilon) * norm_gain[None, :]).astype(jnp.bfloat16)
    gate_act = jnp.dot(
        normed,
        lax.all_gather(gate_weight, "sp", axis=0, tiled=True),
        preferred_element_type=jnp.float32,
    )
    up_act = jnp.dot(
        normed,
        lax.all_gather(up_weight, "sp", axis=0, tiled=True),
        preferred_element_type=jnp.float32,
    )
    hidden = (jax.nn.silu(gate_act) * up_act).astype(jnp.bfloat16)
    partials = jnp.dot(
        hidden,
        lax.all_gather(down_weight, "sp", axis=1, tiled=True),
        preferred_element_type=jnp.float32,
    )
    mlp_out = lax.psum_scatter(
        partials.astype(jnp.bfloat16), "tp", scatter_dimension=1, tiled=True
    ).astype(jnp.float32)
    return (resid.astype(jnp.float32) + mlp_out).astype(jnp.bfloat16)


def remote(src, dst, send, recv, where):
    return pltpu.make_async_remote_copy(
        src_ref=src,
        dst_ref=dst,
        send_sem=send,
        recv_sem=recv,
        device_id=where,
        device_id_type=pl.DeviceIdType.MESH,
    )


def greet(peers):
    barrier = pltpu.get_barrier_semaphore()
    for where in peers:
        pl.semaphore_signal(
            barrier, inc=1, device_id=where, device_id_type=pl.DeviceIdType.MESH
        )
    pl.semaphore_wait(barrier, len(peers))


def neighbours(n_sp, n_tp):
    s, t = lax.axis_index("sp"), lax.axis_index("tp")
    y_peer = s + 1 - 2 * lax.rem(s, 2)
    sibling = t + 1 - 2 * lax.rem(t, 2)
    across = lax.rem(t + 2, n_tp)
    return s, t, y_peer, sibling, across


def front_kernel(
    n_sp, n_tp, w_ref, kv_ref, q1_ref, q2_ref, lam_ref, hgain_ref, ow_ref, res_ref, gain_ref,
    out_ref,
    wall, resid_ref, nall, part2, ybuf, cbuf, zbuf, fbuf,
    kvall, top, low, acc, part_ref, pbuf, rbuf, nbuf, *sems,
):
    (h_s, h_r, v_s, v_r, a_s, a_r, x_s, x_r, c_s, c_r, f_s, f_r, loc,
     p_s, p_r, r_s, r_r, z_s, z_r, y_s, y_r, e_s, e_r, g_s, g_r, o_s, o_r) = sems
    s, t, y_peer, sibling, across = neighbours(n_sp, n_tp)
    z, y = lax.div(s, 2), lax.rem(s, 2)
    half = n_sp // 2
    rows = kv_ref.shape[0]
    part = w_ref.shape[1] // n_sp
    depth = w_ref.shape[2]
    greet(
        [{"sp": lax.rem(s + i, n_sp)} for i in range(1, n_sp)]
        + [{"tp": lax.rem(t + j, n_tp)} for j in range(1, n_tp)]
    )

    def block(who, source):
        return wall.at[:, who, :, pl.ds(pl.multiple_of(source * depth, depth), depth)]

    def piece(dest):
        return w_ref.at[:, pl.ds(pl.multiple_of(dest * part, 16), part), :]

    def weight(i):
        p = lax.rem(s + i, n_sp)
        return remote(piece(p), block(t, s), a_s.at[i - 1], a_r.at[i - 1], {"sp": p})

    def kv_rows(who):
        return kvall.at[pl.ds(pl.multiple_of(who * rows, rows), rows), :]

    def hop(j):
        who = s - 2 * j
        src = kv_ref if j == 0 else kv_rows(who)
        return remote(src, kv_rows(who), h_s.at[j], h_r.at[j], {"sp": lax.rem(s + 2, n_sp)})

    def hop_in(j):
        who = kv_rows(s - 2 - 2 * j)
        return remote(who, who, h_s.at[j], h_r.at[j], {"sp": lax.rem(s + 2, n_sp)})

    def over(j):
        who = s - 2 * j
        src = kv_ref if j == 0 else kv_rows(who)
        return remote(src, kv_rows(who), v_s.at[j], v_r.at[j], {"sp": y_peer})

    def over_in(j):
        who = kv_rows(y_peer - 2 * j)
        return remote(who, who, v_s.at[j], v_r.at[j], {"sp": y_peer})

    own_kv = pltpu.make_async_copy(kv_ref, kv_rows(s), loc.at[0])
    own_kv.start()
    own_w = pltpu.make_async_copy(piece(s), block(t, s), loc.at[1])
    own_w.start()

    @pl.when(z < half - 1)
    def _():
        hop(0).start()

    over(0).start()
    even = list(range(2, n_sp, 2))
    odd = list(range(1, n_sp, 2))
    for i in even:

        @pl.when(s + i >= n_sp)
        def _(i=i):
            weight(i).start()

    for j in range(1, half):

        @pl.when(z >= j)
        def _(j=j):
            hop_in(j - 1).wait_recv()
            if j < half - 1:

                @pl.when(z < half - 1)
                def _():
                    hop(j).start()

            over(j).start()

    for i in even:

        @pl.when(s + i < n_sp)
        def _(i=i):
            weight(i).start()

    for i in odd:
        weight(i).start()

    def across_copy(i):
        source = lax.rem(s - i + n_sp, n_sp)
        return remote(
            block(t, source), block(t, source), x_s.at[i], x_r.at[i], {"tp": across}
        )

    def sibling_copy(i):
        source = lax.rem(s - i + n_sp, n_sp)
        return remote(
            block(t, source), block(t, source), c_s.at[i], c_r.at[i], {"tp": sibling}
        )

    def second_copy(i):
        source = lax.rem(s - i + n_sp, n_sp)
        return remote(
            block(across, source), block(across, source), f_s.at[i], f_r.at[i], {"tp": sibling}
        )

    def relay(i):
        if i == 0:
            own_w.wait()
        else:
            weight(i).wait_recv()
        across_copy(i).start()
        sibling_copy(i).start()

    def second(i):
        across_copy(i).wait_recv()
        second_copy(i).start()

    query_refs = (q1_ref, q2_ref)

    def attend(j):
        first = (z - j) * (2 * rows)
        keys = pl.ds(pl.multiple_of(first, 2 * rows), 2 * rows)
        for c in range(2):
            scores = last_dot(
                query_refs[c][...], kvall[keys, c * HEAD : (c + 1) * HEAD]
            ) * HEAD ** (-0.5)
            if j == 0:
                query_pos = s * rows + lax.broadcasted_iota(jnp.int32, scores.shape, 0)
                key_pos = first + lax.broadcasted_iota(jnp.int32, scores.shape, 1)
                scores = jnp.where(key_pos <= query_pos, scores, masked_score)
            highest = jnp.max(scores, axis=1, keepdims=True)
            if j > 0:
                highest = jnp.maximum(highest, top[c])
            weights_exp = jnp.exp(scores - highest)
            total = jnp.sum(weights_exp, axis=1, keepdims=True)
            weighted = jnp.dot(
                weights_exp.astype(jnp.bfloat16),
                kvall[keys, 2 * HEAD :],
                preferred_element_type=jnp.float32,
            )
            if j > 0:
                keep = jnp.exp(top[c] - highest)
                total = total + keep * low[c]
                weighted = weighted + keep * acc[c]
            top[c] = highest
            low[c] = total
            acc[c] = weighted

    order = [0] + even + odd
    own_kv.wait()
    relay(order[0])
    over_in(0).wait_recv()
    attend(0)
    done, crossed = 1, 0
    for j in range(1, half):
        relay(order[done])
        done += 1

        @pl.when(z >= j)
        def _(j=j):
            over_in(j).wait_recv()
            attend(j)

        second(order[crossed])
        crossed += 1

    mixed = acc[0] / low[0] - lam_ref[0, 0] * acc[1] / low[1]
    mean_square = jnp.mean(mixed * mixed, axis=1, keepdims=True)
    attended = (mixed * lax.rsqrt(mean_square + epsilon) * hgain_ref[...] * 0.8).astype(
        jnp.bfloat16
    )
    width = ow_ref.shape[1]
    for k in range(0, width, 512):
        part_ref[:, k : k + 512] = jnp.dot(
            attended, ow_ref[:, k : k + 512], preferred_element_type=jnp.float32
        ).astype(jnp.bfloat16)

    out_rows = nbuf.shape[0]
    cols = res_ref.shape[1]
    sent = []

    def take(p):
        return pl.ds(pl.multiple_of(p * out_rows, out_rows), out_rows)

    here = pl.ds(pl.multiple_of(t * cols, cols), cols)
    for j in range(1, n_tp):
        p = lax.rem(t + j, n_tp)
        one = remote(part_ref.at[take(p), :], pbuf.at[j - 1], p_s.at[j - 1], p_r.at[j - 1], {"tp": p})
        two = remote(
            res_ref.at[take(p), :], rbuf.at[:, here], r_s.at[j - 1], r_r.at[j - 1], {"tp": p}
        )
        one.start()
        two.start()
        sent += [one, two]
    rbuf[:, here] = res_ref[take(t), :]
    while done < n_sp - 2:
        relay(order[done])
        done += 1
        second(order[crossed])
        crossed += 1
    total = part_ref[take(t), :].astype(jnp.float32)
    for copy in sent:
        copy.wait()
    for j in range(1, n_tp):
        total = total + pbuf[j - 1].astype(jnp.float32)
    resid = (rbuf[...].astype(jnp.float32) + total).astype(jnp.bfloat16)
    resid_ref[...] = resid
    wide = resid.astype(jnp.float32)
    mean = jnp.mean(wide * wide, axis=1, keepdims=True)
    normed = (wide * lax.rsqrt(mean + epsilon) * gain_ref[...]).astype(jnp.bfloat16)
    nbuf[...] = normed
    z_in, y_in = [], []
    copy = remote(nbuf, nall.at[y, z], y_s.at[0], y_r.at[0], {"sp": y_peer})
    copy.start()
    y_in.append(copy)
    for j in range(1, half):
        copy = remote(
            nbuf, nall.at[y, z], z_s.at[j - 1], z_r.at[j - 1], {"sp": lax.rem(s + 2 * j, n_sp)}
        )
        copy.start()
        z_in.append(copy)
    nall[y, z] = normed
    while crossed < n_sp:
        if done < n_sp:
            relay(order[done])
            done += 1
        second(order[crossed])
        crossed += 1
    for j in range(1, half):
        z_in[j - 1].wait_recv()
        held = nall.at[y, lax.rem(z - j + half, half)]
        copy = remote(held, held, y_s.at[j], y_r.at[j], {"sp": y_peer})
        copy.start()
        y_in.append(copy)
    for i in range(n_sp):
        source = lax.rem(s - i + n_sp, n_sp)
        theirs = block(sibling, source)
        remote(theirs, theirs, c_s.at[i], c_r.at[i], {"tp": sibling}).wait_recv()
        theirs = block(lax.rem(sibling + 2, n_tp), source)
        remote(theirs, theirs, f_s.at[i], f_r.at[i], {"tp": sibling}).wait_recv()

    units = n_tp * part

    def mixer(parity, slot):
        tokens = nall[parity].reshape(half * out_rows, width)
        gate_act = last_dot(tokens, wall[0].reshape(units, width))
        up_act = last_dot(tokens, wall[1].reshape(units, width))
        hidden = (gate_act / (1.0 + jnp.exp(-gate_act)) * up_act).astype(jnp.bfloat16)
        for k in range(0, width, 512):
            product = jnp.dot(
                hidden,
                wall[2, :, :, k : k + 512].reshape(units, 512),
                preferred_element_type=jnp.float32,
            ).astype(jnp.bfloat16)
            part2[slot, :, :, k : k + 512] = product.reshape(half, out_rows, 512)

    mixer(y, 0)
    for copy in y_in:
        copy.wait_recv()
    mixer(1 - y, 1)
    turn = list(range(1, half)) + [0]
    e_in = {}
    for j in turn:
        zi = lax.rem(z + j, half)
        copy = remote(part2.at[1, zi], ybuf.at[j], e_s.at[j], e_r.at[j], {"sp": y_peer})
        copy.start()
        e_in[j] = copy
    g_in = []
    for j in turn:
        e_in[j].wait_recv()
        both = part2[0, lax.rem(z + j, half)].astype(jnp.float32) + ybuf[j].astype(jnp.float32)
        if j == 0:
            total = both
        else:
            cbuf[j - 1] = both.astype(jnp.bfloat16)
            copy = remote(
                cbuf.at[j - 1], zbuf.at[j - 1], g_s.at[j - 1], g_r.at[j - 1],
                {"sp": lax.rem(s + 2 * j, n_sp)},
            )
            copy.start()
            g_in.append(copy)
    for copy in g_in:
        copy.wait_recv()
    for j in range(1, half):
        total = total + zbuf[j - 1].astype(jnp.float32)
    fbuf[...] = (resid_ref[...].astype(jnp.float32) + total).astype(jnp.bfloat16)
    o_in = []
    for j in range(1, n_tp):
        p = lax.rem(t + j, n_tp)
        copy = remote(
            fbuf.at[:, pl.ds(pl.multiple_of(p * cols, cols), cols)], out_ref.at[take(t), :],
            o_s.at[j - 1], o_r.at[j - 1], {"tp": p},
        )
        copy.start()
        o_in.append(copy)
    out_ref[take(t), :] = fbuf[:, here]
    for copy in z_in + y_in + g_in:
        copy.wait_send()
    for j in turn:
        e_in[j].wait_send()
    for copy in o_in:
        copy.wait()
    for i in range(n_sp):
        if i > 0:
            weight(i).wait_send()
        across_copy(i).wait_send()
        sibling_copy(i).wait_send()
        second_copy(i).wait_send()
    over(0).wait_send()

    @pl.when(z < half - 1)
    def _():
        hop(0).wait_send()

    for j in range(1, half):

        @pl.when(z >= j)
        def _(j=j):
            over(j).wait_send()
            if j < half - 1:

                @pl.when(z < half - 1)
                def _():
                    hop(j).wait_send()


def front(weights, kv, q1, q2, lam, hgain, ow, res, gain, n_sp, n_tp):
    three, ff_here, depth = weights.shape
    tok, width = kv.shape[0], ow.shape[1]
    rows = tok // n_tp
    half = n_sp // 2
    dma = pltpu.SemaphoreType.DMA
    vmem = pl.BlockSpec(memory_space=pltpu.VMEM)
    bf16, f32 = jnp.bfloat16, jnp.float32
    rowblock = (rows, width)
    return pl.pallas_call(
        functools.partial(front_kernel, n_sp, n_tp),
        out_shape=jax.ShapeDtypeStruct((tok, width // n_tp), bf16),
        in_specs=[vmem] * 4 + [pl.BlockSpec(memory_space=pltpu.SMEM)] + [vmem] * 4,
        out_specs=vmem,
        scratch_shapes=[
            pltpu.VMEM((three, n_tp, ff_here // n_sp, depth * n_sp), bf16),
            pltpu.VMEM(rowblock, bf16),
            pltpu.VMEM((2, half) + rowblock, bf16),
            pltpu.VMEM((2, half) + rowblock, bf16),
            pltpu.VMEM((half,) + rowblock, bf16),
            pltpu.VMEM((half - 1,) + rowblock, bf16),
            pltpu.VMEM((half - 1,) + rowblock, bf16),
            pltpu.VMEM(rowblock, bf16),
            pltpu.VMEM((tok * n_sp, kv.shape[1]), bf16),
            pltpu.VMEM((2, tok, 1), f32),
            pltpu.VMEM((2, tok, 1), f32),
            pltpu.VMEM((2, tok, ow.shape[0]), f32),
            pltpu.VMEM((tok, width), bf16),
            pltpu.VMEM((n_tp - 1,) + rowblock, bf16),
            pltpu.VMEM(rowblock, bf16),
            pltpu.VMEM(rowblock, bf16),
        ]
        + [dma((half,))] * 4
        + [dma((n_sp - 1,))] * 2
        + [dma((n_sp,))] * 6
        + [dma((2,))]
        + [dma((n_tp - 1,))] * 4
        + [dma((half - 1,))] * 2
        + [dma((half,))] * 4
        + [dma((half - 1,))] * 2
        + [dma((n_tp - 1,))] * 2,
        compiler_params=pltpu.CompilerParams(
            collective_id=0, has_side_effects=True, vmem_limit_bytes=56 * 2**20
        ),
        name="front",
    )(weights, kv, q1, q2, lam, hgain, ow, res, gain)


def last_dot(left, right):
    return lax.dot_general(
        left, right, (((1,), (1,)), ((), ())), preferred_element_type=jnp.float32
    )


def split_hidden(
    n_sp,
    n_tp,
    queries_one,
    queries_two,
    keys_one,
    keys_two,
    values,
    mix_lambda,
    head_gain,
    out_weight,
    residual_in,
    norm_gain,
    gate_weight,
    up_weight,
    down_weight,
):
    weights = jnp.stack([gate_weight.T, up_weight.T, down_weight])
    kv = jnp.concatenate([keys_one, keys_two, values], axis=1)
    return front(
        weights,
        kv,
        queries_one,
        queries_two,
        mix_lambda[None, :],
        head_gain[None, :],
        out_weight,
        residual_in,
        norm_gain[None, :],
        n_sp,
        n_tp,
    )


def fits(n_sp, n_tp, shapes):
    tokens, ff, width, heads = shapes
    part = ff // (n_sp * n_tp)
    return (
        n_tp == 4
        and heads == n_tp
        and n_sp % 2 == 0
        and n_sp > 2
        and part % 16 == 0
        and width % (n_sp * 128) == 0
        and tokens % (n_sp * n_tp * 16) == 0
        and tokens * width <= 2**23
    )


def solution(mesh):
    in_specs = (
        P("sp", "tp"),
        P("sp", "tp"),
        P("sp", "tp"),
        P("sp", "tp"),
        P("sp", "tp"),
        P("tp"),
        P("tp"),
        P("tp", None),
        P("sp", "tp"),
        P(),
        P("sp", "tp"),
        P("sp", "tp"),
        P("tp", "sp"),
    )
    out_specs = P("sp", "tp")
    n_sp, n_tp = mesh.shape["sp"], mesh.shape["tp"]

    def layer(*args):
        shapes = (args[0].shape[0], args[10].shape[1], args[10].shape[0], args[5].shape[0])
        body = per_device
        if fits(n_sp, n_tp, shapes):
            body = functools.partial(split_hidden, n_sp, n_tp)
        return jax.shard_map(
            body, mesh=mesh, in_specs=in_specs, out_specs=out_specs, check_vma=False
        )(*args)

    return layer
```

```python
import functools

import jax
import jax.numpy as jnp
from jax import lax
from jax.experimental import pallas as pl
from jax.experimental.pallas import tpu as pltpu
from jax.sharding import PartitionSpec as P

HEAD = 128


epsilon = 1e-06
masked_score = -1e30


def per_device(
    queries_one,
    queries_two,
    keys_one,
    keys_two,
    values,
    mix_lambda,
    head_gain,
    out_weight,
    residual_in,
    norm_gain,
    gate_weight,
    up_weight,
    down_weight,
):
    tok_rows = queries_one.shape[0]
    heads_here = mix_lambda.shape[0]
    head_width = HEAD
    value_width = values.shape[1] // heads_here
    query_pos = lax.axis_index("sp") * tok_rows + jnp.arange(tok_rows, dtype=jnp.int32)
    query_first = queries_one.reshape(tok_rows, heads_here, head_width)
    query_second = queries_two.reshape(tok_rows, heads_here, head_width)
    score_scale = head_width ** (-0.5)

    def update(state, queries, key_rows, value_rows, visible):
        running, totals, weighted = state
        scores = (
            jnp.einsum("qhd,khd->hqk", queries, key_rows, preferred_element_type=jnp.float32)
            * score_scale
        )
        scores = jnp.where(visible[None], scores, masked_score)
        highest = jnp.maximum(running, jnp.max(scores, axis=2))
        weights_exp = jnp.where(visible[None], jnp.exp(scores - highest[..., None]), 0.0)
        totals = jnp.sum(weights_exp, axis=2)
        weighted = jnp.einsum(
            "hqk,khd->hqd",
            weights_exp.astype(jnp.bfloat16),
            value_rows,
            preferred_element_type=jnp.float32,
        )
        return (highest, totals, weighted)

    initial = (
        jnp.full((heads_here, tok_rows), masked_score, jnp.float32),
        jnp.zeros((heads_here, tok_rows), jnp.float32),
        jnp.zeros((heads_here, tok_rows, value_width), jnp.float32),
    )
    key_first = lax.all_gather(keys_one, "sp", axis=0, tiled=True)
    key_second = lax.all_gather(keys_two, "sp", axis=0, tiled=True)
    value_piece = lax.all_gather(values, "sp", axis=0, tiled=True)
    key_count = key_first.shape[0]
    key_pos = jnp.arange(key_count, dtype=jnp.int32)
    visible = key_pos[None, :] <= query_pos[:, None]
    value_rows = value_piece.reshape(key_count, heads_here, value_width)
    first_new = update(
        initial,
        query_first,
        key_first.reshape(key_count, heads_here, head_width),
        value_rows,
        visible,
    )
    second_new = update(
        initial,
        query_second,
        key_second.reshape(key_count, heads_here, head_width),
        value_rows,
        visible,
    )
    lam_heads = mix_lambda[:, None, None]
    mixed = (
        first_new[2] / first_new[1][..., None]
        - lam_heads * second_new[2] / second_new[1][..., None]
    )
    mean_square = jnp.mean(mixed * mixed, axis=2, keepdims=True)
    normed_heads = (
        mixed
        * lax.rsqrt(mean_square + epsilon)
        * head_gain.reshape(heads_here, 1, value_width)
        * 0.8
    )
    attended = (
        normed_heads.transpose(1, 0, 2)
        .reshape(tok_rows, heads_here * value_width)
        .astype(jnp.bfloat16)
    )
    projected = lax.psum_scatter(
        lax.dot_general(
            out_weight, attended, (((0,), (1,)), ((), ())), preferred_element_type=jnp.float32
        ).astype(jnp.bfloat16),
        "tp",
        scatter_dimension=0,
        tiled=True,
    ).astype(jnp.float32)
    resid = (residual_in.astype(jnp.float32) + projected.T).astype(jnp.bfloat16)
    full_rows = lax.all_gather(resid, "tp", axis=1, tiled=True)
    full_float = full_rows.astype(jnp.float32)
    mean_rows = jnp.mean(full_float * full_float, axis=1, keepdims=True)
    normed = (full_float * lax.rsqrt(mean_rows + epsilon) * norm_gain[None, :]).astype(jnp.bfloat16)
    gate_act = jnp.dot(
        normed,
        lax.all_gather(gate_weight, "sp", axis=0, tiled=True),
        preferred_element_type=jnp.float32,
    )
    up_act = jnp.dot(
        normed,
        lax.all_gather(up_weight, "sp", axis=0, tiled=True),
        preferred_element_type=jnp.float32,
    )
    hidden = (jax.nn.silu(gate_act) * up_act).astype(jnp.bfloat16)
    partials = jnp.dot(
        hidden,
        lax.all_gather(down_weight, "sp", axis=1, tiled=True),
        preferred_element_type=jnp.float32,
    )
    mlp_out = lax.psum_scatter(
        partials.astype(jnp.bfloat16), "tp", scatter_dimension=1, tiled=True
    ).astype(jnp.float32)
    return (resid.astype(jnp.float32) + mlp_out).astype(jnp.bfloat16)


def remote(src, dst, send, recv, where):
    return pltpu.make_async_remote_copy(
        src_ref=src,
        dst_ref=dst,
        send_sem=send,
        recv_sem=recv,
        device_id=where,
        device_id_type=pl.DeviceIdType.MESH,
    )


def greet(peers):
    barrier = pltpu.get_barrier_semaphore()
    for where in peers:
        pl.semaphore_signal(
            barrier, inc=1, device_id=where, device_id_type=pl.DeviceIdType.MESH
        )
    pl.semaphore_wait(barrier, len(peers))


def neighbours(n_sp, n_tp):
    s, t = lax.axis_index("sp"), lax.axis_index("tp")
    y_peer = s + 1 - 2 * lax.rem(s, 2)
    sibling = t + 1 - 2 * lax.rem(t, 2)
    across = lax.rem(t + 2, n_tp)
    return s, t, y_peer, sibling, across


def front_kernel(
    n_sp, n_tp, w_ref, kv_ref, q1_ref, q2_ref, lam_ref, hgain_ref, ow_ref, res_ref, gain_ref,
    out_ref,
    wall, resid_ref, nall, hidden, part2, ybuf, cbuf, zbuf, fbuf,
    kvall, top, low, acc, part_ref, pbuf, rbuf, nbuf, *sems,
):
    (h_s, h_r, v_s, v_r, a_s, a_r, x_s, x_r, c_s, c_r, f_s, f_r, loc,
     p_s, p_r, r_s, r_r, z_s, z_r, y_s, y_r, e_s, e_r, g_s, g_r, o_s, o_r) = sems
    s, t, y_peer, sibling, across = neighbours(n_sp, n_tp)
    z, y = lax.div(s, 2), lax.rem(s, 2)
    half = n_sp // 2
    rows = kv_ref.shape[0]
    part = w_ref.shape[1] // n_sp
    depth = w_ref.shape[2]
    greet(
        [{"sp": lax.rem(s + i, n_sp)} for i in range(1, n_sp)]
        + [{"tp": lax.rem(t + j, n_tp)} for j in range(1, n_tp)]
    )

    def block(who, source, w):
        columns = pl.ds(pl.multiple_of(source * depth, depth), depth)
        return wall.at[pl.ds(2 * w, 2 - w), who, :, columns]

    def piece(dest, w):
        units_there = pl.ds(pl.multiple_of(dest * part, 16), part)
        return w_ref.at[pl.ds(2 * w, 2 - w), units_there, :]

    def weight(i, w):
        p = lax.rem(s + i, n_sp)
        return remote(
            piece(p, w), block(t, s, w), a_s.at[w, i - 1], a_r.at[w, i - 1], {"sp": p}
        )

    def kv_rows(who):
        return kvall.at[pl.ds(pl.multiple_of(who * rows, rows), rows), :]

    def hop(j):
        who = s - 2 * j
        src = kv_ref if j == 0 else kv_rows(who)
        return remote(src, kv_rows(who), h_s.at[j], h_r.at[j], {"sp": lax.rem(s + 2, n_sp)})

    def hop_in(j):
        who = kv_rows(s - 2 - 2 * j)
        return remote(who, who, h_s.at[j], h_r.at[j], {"sp": lax.rem(s + 2, n_sp)})

    def over(j):
        who = s - 2 * j
        src = kv_ref if j == 0 else kv_rows(who)
        return remote(src, kv_rows(who), v_s.at[j], v_r.at[j], {"sp": y_peer})

    def over_in(j):
        who = kv_rows(y_peer - 2 * j)
        return remote(who, who, v_s.at[j], v_r.at[j], {"sp": y_peer})

    own_kv = pltpu.make_async_copy(kv_ref, kv_rows(s), loc.at[0])
    own_kv.start()
    own_w = [
        pltpu.make_async_copy(piece(s, w), block(t, s, w), loc.at[1 + w]) for w in range(2)
    ]
    for copy in own_w:
        copy.start()

    @pl.when(z < half - 1)
    def _():
        hop(0).start()

    over(0).start()
    even = list(range(2, n_sp, 2))
    odd = list(range(1, n_sp, 2))
    for i in even:

        @pl.when(s + i >= n_sp)
        def _(i=i):
            weight(i, 0).start()

    for j in range(1, half):

        @pl.when(z >= j)
        def _(j=j):
            hop_in(j - 1).wait_recv()
            if j < half - 1:

                @pl.when(z < half - 1)
                def _():
                    hop(j).start()

            over(j).start()

    for i in even:

        @pl.when(s + i < n_sp)
        def _(i=i):
            weight(i, 0).start()

    for i in odd:
        weight(i, 0).start()

    def across_copy(i, w):
        source = lax.rem(s - i + n_sp, n_sp)
        return remote(
            block(t, source, w), block(t, source, w), x_s.at[w, i], x_r.at[w, i], {"tp": across}
        )

    def sibling_copy(i, w):
        source = lax.rem(s - i + n_sp, n_sp)
        return remote(
            block(t, source, w), block(t, source, w), c_s.at[w, i], c_r.at[w, i], {"tp": sibling}
        )

    def second_copy(i, w):
        held = block(across, lax.rem(s - i + n_sp, n_sp), w)
        return remote(held, held, f_s.at[w, i], f_r.at[w, i], {"tp": sibling})

    def relay(i, w):
        if i == 0:
            own_w[w].wait()
        else:
            weight(i, w).wait_recv()
        across_copy(i, w).start()
        sibling_copy(i, w).start()

    def second(i, w):
        across_copy(i, w).wait_recv()
        second_copy(i, w).start()

    def settle(w):
        for i in range(n_sp):
            source = lax.rem(s - i + n_sp, n_sp)
            theirs = block(sibling, source, w)
            remote(theirs, theirs, c_s.at[w, i], c_r.at[w, i], {"tp": sibling}).wait_recv()
            theirs = block(lax.rem(sibling + 2, n_tp), source, w)
            remote(theirs, theirs, f_s.at[w, i], f_r.at[w, i], {"tp": sibling}).wait_recv()

    query_refs = (q1_ref, q2_ref)

    def attend(j):
        first = (z - j) * (2 * rows)
        keys = pl.ds(pl.multiple_of(first, 2 * rows), 2 * rows)
        for c in range(2):
            scores = last_dot(
                query_refs[c][...], kvall[keys, c * HEAD : (c + 1) * HEAD]
            ) * HEAD ** (-0.5)
            if j == 0:
                query_pos = s * rows + lax.broadcasted_iota(jnp.int32, scores.shape, 0)
                key_pos = first + lax.broadcasted_iota(jnp.int32, scores.shape, 1)
                scores = jnp.where(key_pos <= query_pos, scores, masked_score)
            highest = jnp.max(scores, axis=1, keepdims=True)
            if j > 0:
                highest = jnp.maximum(highest, top[c])
            weights_exp = jnp.exp(scores - highest)
            total = jnp.sum(weights_exp, axis=1, keepdims=True)
            weighted = jnp.dot(
                weights_exp.astype(jnp.bfloat16),
                kvall[keys, 2 * HEAD :],
                preferred_element_type=jnp.float32,
            )
            if j > 0:
                keep = jnp.exp(top[c] - highest)
                total = total + keep * low[c]
                weighted = weighted + keep * acc[c]
            top[c] = highest
            low[c] = total
            acc[c] = weighted

    order = [0] + even + odd
    own_kv.wait()
    relay(order[0], 0)
    over_in(0).wait_recv()
    attend(0)
    for j in range(1, half):

        @pl.when(z >= j)
        def _(j=j):
            over_in(j).wait_recv()
            attend(j)

        relay(order[j], 0)
        second(order[j - 1], 0)

    mixed = acc[0] / low[0] - lam_ref[0, 0] * acc[1] / low[1]
    mean_square = jnp.mean(mixed * mixed, axis=1, keepdims=True)
    attended = (mixed * lax.rsqrt(mean_square + epsilon) * hgain_ref[...] * 0.8).astype(
        jnp.bfloat16
    )
    width = ow_ref.shape[1]
    for k in range(0, width, 512):
        part_ref[:, k : k + 512] = jnp.dot(
            attended, ow_ref[:, k : k + 512], preferred_element_type=jnp.float32
        ).astype(jnp.bfloat16)

    out_rows = nbuf.shape[0]
    cols = res_ref.shape[1]
    sent = []

    def take(p):
        return pl.ds(pl.multiple_of(p * out_rows, out_rows), out_rows)

    here = pl.ds(pl.multiple_of(t * cols, cols), cols)
    for j in range(1, n_tp):
        p = lax.rem(t + j, n_tp)
        one = remote(part_ref.at[take(p), :], pbuf.at[j - 1], p_s.at[j - 1], p_r.at[j - 1], {"tp": p})
        two = remote(
            res_ref.at[take(p), :], rbuf.at[:, here], r_s.at[j - 1], r_r.at[j - 1], {"tp": p}
        )
        one.start()
        two.start()
        sent += [one, two]
    rbuf[:, here] = res_ref[take(t), :]
    total = part_ref[take(t), :].astype(jnp.float32)
    for copy in sent:
        copy.wait()
    for j in range(1, n_tp):
        total = total + pbuf[j - 1].astype(jnp.float32)
    resid = (rbuf[...].astype(jnp.float32) + total).astype(jnp.bfloat16)
    resid_ref[...] = resid
    wide = resid.astype(jnp.float32)
    mean = jnp.mean(wide * wide, axis=1, keepdims=True)
    normed = (wide * lax.rsqrt(mean + epsilon) * gain_ref[...]).astype(jnp.bfloat16)
    nbuf[...] = normed
    z_in, y_in = [], []
    copy = remote(nbuf, nall.at[y, z], y_s.at[0], y_r.at[0], {"sp": y_peer})
    copy.start()
    y_in.append(copy)
    for j in range(1, half):
        copy = remote(
            nbuf, nall.at[y, z], z_s.at[j - 1], z_r.at[j - 1], {"sp": lax.rem(s + 2 * j, n_sp)}
        )
        copy.start()
        z_in.append(copy)
    nall[y, z] = normed
    for i in even + odd:
        weight(i, 1).start()
    for k in range(half, n_sp):
        relay(order[k], 0)
        second(order[k - 1], 0)
    second(order[n_sp - 1], 0)
    for j in range(1, half):
        z_in[j - 1].wait_recv()
        held = nall.at[y, lax.rem(z - j + half, half)]
        copy = remote(held, held, y_s.at[j], y_r.at[j], {"sp": y_peer})
        copy.start()
        y_in.append(copy)
    settle(0)
    units = n_tp * part

    def gated(parity, slot):
        tokens = nall[parity].reshape(half * out_rows, width)
        gate_act = last_dot(tokens, wall[0].reshape(units, width))
        up_act = last_dot(tokens, wall[1].reshape(units, width))
        hidden[slot] = (gate_act / (1.0 + jnp.exp(-gate_act)) * up_act).astype(jnp.bfloat16)

    def down(slot):
        for k in range(0, width, 512):
            product = jnp.dot(
                hidden[slot],
                wall[2, :, :, k : k + 512].reshape(units, 512),
                preferred_element_type=jnp.float32,
            ).astype(jnp.bfloat16)
            part2[slot, :, :, k : k + 512] = product.reshape(half, out_rows, 512)

    gated(y, 0)
    relay(order[0], 1)
    for k in range(1, half):
        relay(order[k], 1)
        second(order[k - 1], 1)
    for copy in y_in:
        copy.wait_recv()
    gated(1 - y, 1)
    for k in range(half, n_sp):
        relay(order[k], 1)
        second(order[k - 1], 1)
    second(order[n_sp - 1], 1)
    settle(1)
    down(1)
    turn = list(range(1, half)) + [0]
    e_in = {}
    for j in turn:
        zi = lax.rem(z + j, half)
        copy = remote(part2.at[1, zi], ybuf.at[j], e_s.at[j], e_r.at[j], {"sp": y_peer})
        copy.start()
        e_in[j] = copy
    down(0)
    g_in = []
    for j in turn:
        e_in[j].wait_recv()
        both = part2[0, lax.rem(z + j, half)].astype(jnp.float32) + ybuf[j].astype(jnp.float32)
        if j == 0:
            total = both
        else:
            cbuf[j - 1] = both.astype(jnp.bfloat16)
            copy = remote(
                cbuf.at[j - 1], zbuf.at[j - 1], g_s.at[j - 1], g_r.at[j - 1],
                {"sp": lax.rem(s + 2 * j, n_sp)},
            )
            copy.start()
            g_in.append(copy)
    for copy in g_in:
        copy.wait_recv()
    for j in range(1, half):
        total = total + zbuf[j - 1].astype(jnp.float32)
    fbuf[...] = (resid_ref[...].astype(jnp.float32) + total).astype(jnp.bfloat16)
    o_in = []
    for j in range(1, n_tp):
        p = lax.rem(t + j, n_tp)
        copy = remote(
            fbuf.at[:, pl.ds(pl.multiple_of(p * cols, cols), cols)], out_ref.at[take(t), :],
            o_s.at[j - 1], o_r.at[j - 1], {"tp": p},
        )
        copy.start()
        o_in.append(copy)
    out_ref[take(t), :] = fbuf[:, here]
    for copy in z_in + y_in + g_in:
        copy.wait_send()
    for j in turn:
        e_in[j].wait_send()
    for copy in o_in:
        copy.wait()
    for w in range(2):
        for i in range(n_sp):
            if i > 0:
                weight(i, w).wait_send()
            across_copy(i, w).wait_send()
            sibling_copy(i, w).wait_send()
            second_copy(i, w).wait_send()
    over(0).wait_send()

    @pl.when(z < half - 1)
    def _():
        hop(0).wait_send()

    for j in range(1, half):

        @pl.when(z >= j)
        def _(j=j):
            over(j).wait_send()
            if j < half - 1:

                @pl.when(z < half - 1)
                def _():
                    hop(j).wait_send()


def front(weights, kv, q1, q2, lam, hgain, ow, res, gain, n_sp, n_tp):
    three, ff_here, depth = weights.shape
    tok, width = kv.shape[0], ow.shape[1]
    rows = tok // n_tp
    half = n_sp // 2
    dma = pltpu.SemaphoreType.DMA
    vmem = pl.BlockSpec(memory_space=pltpu.VMEM)
    bf16, f32 = jnp.bfloat16, jnp.float32
    rowblock = (rows, width)
    return pl.pallas_call(
        functools.partial(front_kernel, n_sp, n_tp),
        out_shape=jax.ShapeDtypeStruct((tok, width // n_tp), bf16),
        in_specs=[vmem] * 4 + [pl.BlockSpec(memory_space=pltpu.SMEM)] + [vmem] * 4,
        out_specs=vmem,
        scratch_shapes=[
            pltpu.VMEM((three, n_tp, ff_here // n_sp, depth * n_sp), bf16),
            pltpu.VMEM(rowblock, bf16),
            pltpu.VMEM((2, half) + rowblock, bf16),
            pltpu.VMEM((2, half * rows, n_tp * (ff_here // n_sp)), bf16),
            pltpu.VMEM((2, half) + rowblock, bf16),
            pltpu.VMEM((half,) + rowblock, bf16),
            pltpu.VMEM((half - 1,) + rowblock, bf16),
            pltpu.VMEM((half - 1,) + rowblock, bf16),
            pltpu.VMEM(rowblock, bf16),
            pltpu.VMEM((tok * n_sp, kv.shape[1]), bf16),
            pltpu.VMEM((2, tok, 1), f32),
            pltpu.VMEM((2, tok, 1), f32),
            pltpu.VMEM((2, tok, ow.shape[0]), f32),
            pltpu.VMEM((tok, width), bf16),
            pltpu.VMEM((n_tp - 1,) + rowblock, bf16),
            pltpu.VMEM(rowblock, bf16),
            pltpu.VMEM(rowblock, bf16),
        ]
        + [dma((half,))] * 4
        + [dma((2, n_sp - 1))] * 2
        + [dma((2, n_sp))] * 6
        + [dma((3,))]
        + [dma((n_tp - 1,))] * 4
        + [dma((half - 1,))] * 2
        + [dma((half,))] * 4
        + [dma((half - 1,))] * 2
        + [dma((n_tp - 1,))] * 2,
        compiler_params=pltpu.CompilerParams(
            collective_id=0, has_side_effects=True, vmem_limit_bytes=56 * 2**20
        ),
        name="front",
    )(weights, kv, q1, q2, lam, hgain, ow, res, gain)


def last_dot(left, right):
    return lax.dot_general(
        left, right, (((1,), (1,)), ((), ())), preferred_element_type=jnp.float32
    )


def split_hidden(
    n_sp,
    n_tp,
    queries_one,
    queries_two,
    keys_one,
    keys_two,
    values,
    mix_lambda,
    head_gain,
    out_weight,
    residual_in,
    norm_gain,
    gate_weight,
    up_weight,
    down_weight,
):
    weights = jnp.stack([gate_weight.T, up_weight.T, down_weight])
    kv = jnp.concatenate([keys_one, keys_two, values], axis=1)
    return front(
        weights,
        kv,
        queries_one,
        queries_two,
        mix_lambda[None, :],
        head_gain[None, :],
        out_weight,
        residual_in,
        norm_gain[None, :],
        n_sp,
        n_tp,
    )


def fits(n_sp, n_tp, shapes):
    tokens, ff, width, heads = shapes
    part = ff // (n_sp * n_tp)
    return (
        n_tp == 4
        and heads == n_tp
        and n_sp % 2 == 0
        and n_sp > 2
        and part % 16 == 0
        and width % (n_sp * 128) == 0
        and tokens % (n_sp * n_tp * 16) == 0
        and tokens * width <= 2**23
    )


def solution(mesh):
    in_specs = (
        P("sp", "tp"),
        P("sp", "tp"),
        P("sp", "tp"),
        P("sp", "tp"),
        P("sp", "tp"),
        P("tp"),
        P("tp"),
        P("tp", None),
        P("sp", "tp"),
        P(),
        P("sp", "tp"),
        P("sp", "tp"),
        P("tp", "sp"),
    )
    out_specs = P("sp", "tp")
    n_sp, n_tp = mesh.shape["sp"], mesh.shape["tp"]

    def layer(*args):
        shapes = (args[0].shape[0], args[10].shape[1], args[10].shape[0], args[5].shape[0])
        body = per_device
        if fits(n_sp, n_tp, shapes):
            body = functools.partial(split_hidden, n_sp, n_tp)
        return jax.shard_map(
            body, mesh=mesh, in_specs=in_specs, out_specs=out_specs, check_vma=False
        )(*args)

    return layer
```

```python
import functools

import jax
import jax.numpy as jnp
from jax import lax
from jax.experimental import pallas as pl
from jax.experimental.pallas import tpu as pltpu
from jax.sharding import PartitionSpec as P

HEAD = 128


epsilon = 1e-06
masked_score = -1e30


def per_device(
    queries_one,
    queries_two,
    keys_one,
    keys_two,
    values,
    mix_lambda,
    head_gain,
    out_weight,
    residual_in,
    norm_gain,
    gate_weight,
    up_weight,
    down_weight,
):
    tok_rows = queries_one.shape[0]
    heads_here = mix_lambda.shape[0]
    head_width = HEAD
    value_width = values.shape[1] // heads_here
    query_pos = lax.axis_index("sp") * tok_rows + jnp.arange(tok_rows, dtype=jnp.int32)
    query_first = queries_one.reshape(tok_rows, heads_here, head_width)
    query_second = queries_two.reshape(tok_rows, heads_here, head_width)
    score_scale = head_width ** (-0.5)

    def update(state, queries, key_rows, value_rows, visible):
        running, totals, weighted = state
        scores = (
            jnp.einsum("qhd,khd->hqk", queries, key_rows, preferred_element_type=jnp.float32)
            * score_scale
        )
        scores = jnp.where(visible[None], scores, masked_score)
        highest = jnp.maximum(running, jnp.max(scores, axis=2))
        weights_exp = jnp.where(visible[None], jnp.exp(scores - highest[..., None]), 0.0)
        totals = jnp.sum(weights_exp, axis=2)
        weighted = jnp.einsum(
            "hqk,khd->hqd",
            weights_exp.astype(jnp.bfloat16),
            value_rows,
            preferred_element_type=jnp.float32,
        )
        return (highest, totals, weighted)

    initial = (
        jnp.full((heads_here, tok_rows), masked_score, jnp.float32),
        jnp.zeros((heads_here, tok_rows), jnp.float32),
        jnp.zeros((heads_here, tok_rows, value_width), jnp.float32),
    )
    key_first = lax.all_gather(keys_one, "sp", axis=0, tiled=True)
    key_second = lax.all_gather(keys_two, "sp", axis=0, tiled=True)
    value_piece = lax.all_gather(values, "sp", axis=0, tiled=True)
    key_count = key_first.shape[0]
    key_pos = jnp.arange(key_count, dtype=jnp.int32)
    visible = key_pos[None, :] <= query_pos[:, None]
    value_rows = value_piece.reshape(key_count, heads_here, value_width)
    first_new = update(
        initial,
        query_first,
        key_first.reshape(key_count, heads_here, head_width),
        value_rows,
        visible,
    )
    second_new = update(
        initial,
        query_second,
        key_second.reshape(key_count, heads_here, head_width),
        value_rows,
        visible,
    )
    lam_heads = mix_lambda[:, None, None]
    mixed = (
        first_new[2] / first_new[1][..., None]
        - lam_heads * second_new[2] / second_new[1][..., None]
    )
    mean_square = jnp.mean(mixed * mixed, axis=2, keepdims=True)
    normed_heads = (
        mixed
        * lax.rsqrt(mean_square + epsilon)
        * head_gain.reshape(heads_here, 1, value_width)
        * 0.8
    )
    attended = (
        normed_heads.transpose(1, 0, 2)
        .reshape(tok_rows, heads_here * value_width)
        .astype(jnp.bfloat16)
    )
    projected = lax.psum_scatter(
        lax.dot_general(
            out_weight, attended, (((0,), (1,)), ((), ())), preferred_element_type=jnp.float32
        ).astype(jnp.bfloat16),
        "tp",
        scatter_dimension=0,
        tiled=True,
    ).astype(jnp.float32)
    resid = (residual_in.astype(jnp.float32) + projected.T).astype(jnp.bfloat16)
    full_rows = lax.all_gather(resid, "tp", axis=1, tiled=True)
    full_float = full_rows.astype(jnp.float32)
    mean_rows = jnp.mean(full_float * full_float, axis=1, keepdims=True)
    normed = (full_float * lax.rsqrt(mean_rows + epsilon) * norm_gain[None, :]).astype(jnp.bfloat16)
    gate_act = jnp.dot(
        normed,
        lax.all_gather(gate_weight, "sp", axis=0, tiled=True),
        preferred_element_type=jnp.float32,
    )
    up_act = jnp.dot(
        normed,
        lax.all_gather(up_weight, "sp", axis=0, tiled=True),
        preferred_element_type=jnp.float32,
    )
    hidden = (jax.nn.silu(gate_act) * up_act).astype(jnp.bfloat16)
    partials = jnp.dot(
        hidden,
        lax.all_gather(down_weight, "sp", axis=1, tiled=True),
        preferred_element_type=jnp.float32,
    )
    mlp_out = lax.psum_scatter(
        partials.astype(jnp.bfloat16), "tp", scatter_dimension=1, tiled=True
    ).astype(jnp.float32)
    return (resid.astype(jnp.float32) + mlp_out).astype(jnp.bfloat16)


def remote(src, dst, send, recv, where):
    return pltpu.make_async_remote_copy(
        src_ref=src,
        dst_ref=dst,
        send_sem=send,
        recv_sem=recv,
        device_id=where,
        device_id_type=pl.DeviceIdType.MESH,
    )


def greet(peers):
    barrier = pltpu.get_barrier_semaphore()
    for where in peers:
        pl.semaphore_signal(
            barrier, inc=1, device_id=where, device_id_type=pl.DeviceIdType.MESH
        )
    pl.semaphore_wait(barrier, len(peers))


def neighbours(n_sp, n_tp):
    s, t = lax.axis_index("sp"), lax.axis_index("tp")
    y_peer = s + 1 - 2 * lax.rem(s, 2)
    sibling = t + 1 - 2 * lax.rem(t, 2)
    across = lax.rem(t + 2, n_tp)
    return s, t, y_peer, sibling, across


def front_kernel(
    n_sp, n_tp, w_ref, kv_ref, q1_ref, q2_ref, lam_ref, hgain_ref, ow_ref, res_ref, gain_ref,
    out_ref,
    wall, resid_ref, nall, part2, ybuf, cbuf, zbuf, fbuf,
    kvall, top, low, acc, part_ref, pbuf, rbuf, nbuf, *sems,
):
    (h_s, h_r, v_s, v_r, a_s, a_r, x_s, x_r, c_s, c_r, f_s, f_r, loc,
     p_s, p_r, r_s, r_r, z_s, z_r, y_s, y_r, e_s, e_r, g_s, g_r, o_s, o_r) = sems
    s, t, y_peer, sibling, across = neighbours(n_sp, n_tp)
    z, y = lax.div(s, 2), lax.rem(s, 2)
    half = n_sp // 2
    rows = kv_ref.shape[0]
    part = w_ref.shape[1] // n_sp
    depth = w_ref.shape[2]
    greet(
        [{"sp": lax.rem(s + i, n_sp)} for i in range(1, n_sp)]
        + [{"tp": lax.rem(t + j, n_tp)} for j in range(1, n_tp)]
    )

    def block(who, source):
        return wall.at[:, who, :, pl.ds(pl.multiple_of(source * depth, depth), depth)]

    def piece(dest):
        return w_ref.at[:, pl.ds(pl.multiple_of(dest * part, 16), part), :]

    def weight(i):
        p = lax.rem(s + i, n_sp)
        return remote(piece(p), block(t, s), a_s.at[i - 1], a_r.at[i - 1], {"sp": p})

    def kv_rows(who):
        return kvall.at[pl.ds(pl.multiple_of(who * rows, rows), rows), :]

    def hop(j):
        who = s - 2 * j
        src = kv_ref if j == 0 else kv_rows(who)
        return remote(src, kv_rows(who), h_s.at[j], h_r.at[j], {"sp": lax.rem(s + 2, n_sp)})

    def hop_in(j):
        who = kv_rows(s - 2 - 2 * j)
        return remote(who, who, h_s.at[j], h_r.at[j], {"sp": lax.rem(s + 2, n_sp)})

    def over(j):
        who = s - 2 * j
        src = kv_ref if j == 0 else kv_rows(who)
        return remote(src, kv_rows(who), v_s.at[j], v_r.at[j], {"sp": y_peer})

    def over_in(j):
        who = kv_rows(y_peer - 2 * j)
        return remote(who, who, v_s.at[j], v_r.at[j], {"sp": y_peer})

    own_kv = pltpu.make_async_copy(kv_ref, kv_rows(s), loc.at[0])
    own_kv.start()
    own_w = pltpu.make_async_copy(piece(s), block(t, s), loc.at[1])
    own_w.start()

    @pl.when(z < half - 1)
    def _():
        hop(0).start()

    over(0).start()
    even = list(range(2, n_sp, 2))
    odd = list(range(1, n_sp, 2))
    for i in even:

        @pl.when(s + i >= n_sp)
        def _(i=i):
            weight(i).start()

    for j in range(1, half):

        @pl.when(z >= j)
        def _(j=j):
            hop_in(j - 1).wait_recv()
            if j < half - 1:

                @pl.when(z < half - 1)
                def _():
                    hop(j).start()

            over(j).start()

    for i in even:

        @pl.when(s + i < n_sp)
        def _(i=i):
            weight(i).start()

    for i in odd:
        weight(i).start()

    def across_copy(i):
        source = lax.rem(s - i + n_sp, n_sp)
        return remote(
            block(t, source), block(t, source), x_s.at[i], x_r.at[i], {"tp": across}
        )

    def sibling_copy(i):
        source = lax.rem(s - i + n_sp, n_sp)
        return remote(
            block(t, source), block(t, source), c_s.at[i], c_r.at[i], {"tp": sibling}
        )

    def second_copy(i):
        source = lax.rem(s - i + n_sp, n_sp)
        return remote(
            block(across, source), block(across, source), f_s.at[i], f_r.at[i], {"tp": sibling}
        )

    def relay(i):
        if i == 0:
            own_w.wait()
        else:
            weight(i).wait_recv()
        across_copy(i).start()
        sibling_copy(i).start()

    def second(i):
        across_copy(i).wait_recv()
        second_copy(i).start()

    query_refs = (q1_ref, q2_ref)

    def attend(j):
        first = (z - j) * (2 * rows)
        keys = pl.ds(pl.multiple_of(first, 2 * rows), 2 * rows)
        for c in range(2):
            scores = last_dot(
                query_refs[c][...], kvall[keys, c * HEAD : (c + 1) * HEAD]
            ) * HEAD ** (-0.5)
            if j == 0:
                query_pos = s * rows + lax.broadcasted_iota(jnp.int32, scores.shape, 0)
                key_pos = first + lax.broadcasted_iota(jnp.int32, scores.shape, 1)
                scores = jnp.where(key_pos <= query_pos, scores, masked_score)
            highest = jnp.max(scores, axis=1, keepdims=True)
            if j > 0:
                highest = jnp.maximum(highest, top[c])
            weights_exp = jnp.exp(scores - highest)
            total = jnp.sum(weights_exp, axis=1, keepdims=True)
            weighted = jnp.dot(
                weights_exp.astype(jnp.bfloat16),
                kvall[keys, 2 * HEAD :],
                preferred_element_type=jnp.float32,
            )
            if j > 0:
                keep = jnp.exp(top[c] - highest)
                total = total + keep * low[c]
                weighted = weighted + keep * acc[c]
            top[c] = highest
            low[c] = total
            acc[c] = weighted

    order = [0] + even + odd
    own_kv.wait()
    relay(order[0])
    over_in(0).wait_recv()
    attend(0)
    done, crossed = 1, 0
    for j in range(1, half):

        @pl.when(z >= j)
        def _(j=j):
            over_in(j).wait_recv()
            attend(j)

        relay(order[done])
        done += 1
        second(order[crossed])
        crossed += 1

    mixed = acc[0] / low[0] - lam_ref[0, 0] * acc[1] / low[1]
    mean_square = jnp.mean(mixed * mixed, axis=1, keepdims=True)
    attended = (mixed * lax.rsqrt(mean_square + epsilon) * hgain_ref[...] * 0.8).astype(
        jnp.bfloat16
    )
    width = ow_ref.shape[1]
    for k in range(0, width, 512):
        part_ref[:, k : k + 512] = jnp.dot(
            attended, ow_ref[:, k : k + 512], preferred_element_type=jnp.float32
        ).astype(jnp.bfloat16)

    out_rows = nbuf.shape[0]
    cols = res_ref.shape[1]
    sent = []

    def take(p):
        return pl.ds(pl.multiple_of(p * out_rows, out_rows), out_rows)

    here = pl.ds(pl.multiple_of(t * cols, cols), cols)
    for j in range(1, n_tp):
        p = lax.rem(t + j, n_tp)
        one = remote(part_ref.at[take(p), :], pbuf.at[j - 1], p_s.at[j - 1], p_r.at[j - 1], {"tp": p})
        two = remote(
            res_ref.at[take(p), :], rbuf.at[:, here], r_s.at[j - 1], r_r.at[j - 1], {"tp": p}
        )
        one.start()
        two.start()
        sent += [one, two]
    rbuf[:, here] = res_ref[take(t), :]
    total = part_ref[take(t), :].astype(jnp.float32)
    for copy in sent:
        copy.wait()
    for j in range(1, n_tp):
        total = total + pbuf[j - 1].astype(jnp.float32)
    resid = (rbuf[...].astype(jnp.float32) + total).astype(jnp.bfloat16)
    resid_ref[...] = resid
    wide = resid.astype(jnp.float32)
    mean = jnp.mean(wide * wide, axis=1, keepdims=True)
    normed = (wide * lax.rsqrt(mean + epsilon) * gain_ref[...]).astype(jnp.bfloat16)
    nbuf[...] = normed
    z_in, y_in = [], []
    copy = remote(nbuf, nall.at[y, z], y_s.at[0], y_r.at[0], {"sp": y_peer})
    copy.start()
    y_in.append(copy)
    for j in range(1, half):
        copy = remote(
            nbuf, nall.at[y, z], z_s.at[j - 1], z_r.at[j - 1], {"sp": lax.rem(s + 2 * j, n_sp)}
        )
        copy.start()
        z_in.append(copy)
    nall[y, z] = normed
    while crossed < n_sp:
        if done < n_sp:
            relay(order[done])
            done += 1
        second(order[crossed])
        crossed += 1
    for j in range(1, half):
        z_in[j - 1].wait_recv()
        held = nall.at[y, lax.rem(z - j + half, half)]
        copy = remote(held, held, y_s.at[j], y_r.at[j], {"sp": y_peer})
        copy.start()
        y_in.append(copy)
    for i in range(n_sp):
        source = lax.rem(s - i + n_sp, n_sp)
        theirs = block(sibling, source)
        remote(theirs, theirs, c_s.at[i], c_r.at[i], {"tp": sibling}).wait_recv()
        theirs = block(lax.rem(sibling + 2, n_tp), source)
        remote(theirs, theirs, f_s.at[i], f_r.at[i], {"tp": sibling}).wait_recv()

    units = n_tp * part

    def mixer(parity, slot):
        tokens = nall[parity].reshape(half * out_rows, width)
        gate_act = last_dot(tokens, wall[0].reshape(units, width))
        up_act = last_dot(tokens, wall[1].reshape(units, width))
        hidden = (gate_act / (1.0 + jnp.exp(-gate_act)) * up_act).astype(jnp.bfloat16)
        for k in range(0, width, 512):
            product = jnp.dot(
                hidden,
                wall[2, :, :, k : k + 512].reshape(units, 512),
                preferred_element_type=jnp.float32,
            ).astype(jnp.bfloat16)
            part2[slot, :, :, k : k + 512] = product.reshape(half, out_rows, 512)

    mixer(y, 0)
    for copy in y_in:
        copy.wait_recv()
    mixer(1 - y, 1)
    turn = list(range(1, half)) + [0]
    e_in = {}
    for j in turn:
        zi = lax.rem(z + j, half)
        copy = remote(part2.at[1, zi], ybuf.at[j], e_s.at[j], e_r.at[j], {"sp": y_peer})
        copy.start()
        e_in[j] = copy
    g_in = []
    for j in turn:
        e_in[j].wait_recv()
        both = part2[0, lax.rem(z + j, half)].astype(jnp.float32) + ybuf[j].astype(jnp.float32)
        if j == 0:
            total = both
        else:
            cbuf[j - 1] = both.astype(jnp.bfloat16)
            copy = remote(
                cbuf.at[j - 1], zbuf.at[j - 1], g_s.at[j - 1], g_r.at[j - 1],
                {"sp": lax.rem(s + 2 * j, n_sp)},
            )
            copy.start()
            g_in.append(copy)
    for copy in g_in:
        copy.wait_recv()
    for j in range(1, half):
        total = total + zbuf[j - 1].astype(jnp.float32)
    fbuf[...] = (resid_ref[...].astype(jnp.float32) + total).astype(jnp.bfloat16)
    o_in = []
    for j in range(1, n_tp):
        p = lax.rem(t + j, n_tp)
        copy = remote(
            fbuf.at[:, pl.ds(pl.multiple_of(p * cols, cols), cols)], out_ref.at[take(t), :],
            o_s.at[j - 1], o_r.at[j - 1], {"tp": p},
        )
        copy.start()
        o_in.append(copy)
    out_ref[take(t), :] = fbuf[:, here]
    for copy in z_in + y_in + g_in:
        copy.wait_send()
    for j in turn:
        e_in[j].wait_send()
    for copy in o_in:
        copy.wait()
    for i in range(n_sp):
        if i > 0:
            weight(i).wait_send()
        across_copy(i).wait_send()
        sibling_copy(i).wait_send()
        second_copy(i).wait_send()
    over(0).wait_send()

    @pl.when(z < half - 1)
    def _():
        hop(0).wait_send()

    for j in range(1, half):

        @pl.when(z >= j)
        def _(j=j):
            over(j).wait_send()
            if j < half - 1:

                @pl.when(z < half - 1)
                def _():
                    hop(j).wait_send()


def front(weights, kv, q1, q2, lam, hgain, ow, res, gain, n_sp, n_tp):
    three, ff_here, depth = weights.shape
    tok, width = kv.shape[0], ow.shape[1]
    rows = tok // n_tp
    half = n_sp // 2
    dma = pltpu.SemaphoreType.DMA
    vmem = pl.BlockSpec(memory_space=pltpu.VMEM)
    bf16, f32 = jnp.bfloat16, jnp.float32
    rowblock = (rows, width)
    return pl.pallas_call(
        functools.partial(front_kernel, n_sp, n_tp),
        out_shape=jax.ShapeDtypeStruct((tok, width // n_tp), bf16),
        in_specs=[vmem] * 4 + [pl.BlockSpec(memory_space=pltpu.SMEM)] + [vmem] * 4,
        out_specs=vmem,
        scratch_shapes=[
            pltpu.VMEM((three, n_tp, ff_here // n_sp, depth * n_sp), bf16),
            pltpu.VMEM(rowblock, bf16),
            pltpu.VMEM((2, half) + rowblock, bf16),
            pltpu.VMEM((2, half) + rowblock, bf16),
            pltpu.VMEM((half,) + rowblock, bf16),
            pltpu.VMEM((half - 1,) + rowblock, bf16),
            pltpu.VMEM((half - 1,) + rowblock, bf16),
            pltpu.VMEM(rowblock, bf16),
            pltpu.VMEM((tok * n_sp, kv.shape[1]), bf16),
            pltpu.VMEM((2, tok, 1), f32),
            pltpu.VMEM((2, tok, 1), f32),
            pltpu.VMEM((2, tok, ow.shape[0]), f32),
            pltpu.VMEM((tok, width), bf16),
            pltpu.VMEM((n_tp - 1,) + rowblock, bf16),
            pltpu.VMEM(rowblock, bf16),
            pltpu.VMEM(rowblock, bf16),
        ]
        + [dma((half,))] * 4
        + [dma((n_sp - 1,))] * 2
        + [dma((n_sp,))] * 6
        + [dma((2,))]
        + [dma((n_tp - 1,))] * 4
        + [dma((half - 1,))] * 2
        + [dma((half,))] * 4
        + [dma((half - 1,))] * 2
        + [dma((n_tp - 1,))] * 2,
        compiler_params=pltpu.CompilerParams(
            collective_id=0, has_side_effects=True, vmem_limit_bytes=56 * 2**20
        ),
        name="front",
    )(weights, kv, q1, q2, lam, hgain, ow, res, gain)


def last_dot(left, right):
    return lax.dot_general(
        left, right, (((1,), (1,)), ((), ())), preferred_element_type=jnp.float32
    )


def split_hidden(
    n_sp,
    n_tp,
    queries_one,
    queries_two,
    keys_one,
    keys_two,
    values,
    mix_lambda,
    head_gain,
    out_weight,
    residual_in,
    norm_gain,
    gate_weight,
    up_weight,
    down_weight,
):
    weights = jnp.stack([gate_weight.T, up_weight.T, down_weight])
    kv = jnp.concatenate([keys_one, keys_two, values], axis=1)
    return front(
        weights,
        kv,
        queries_one,
        queries_two,
        mix_lambda[None, :],
        head_gain[None, :],
        out_weight,
        residual_in,
        norm_gain[None, :],
        n_sp,
        n_tp,
    )


def fits(n_sp, n_tp, shapes):
    tokens, ff, width, heads = shapes
    part = ff // (n_sp * n_tp)
    return (
        n_tp == 4
        and heads == n_tp
        and n_sp % 2 == 0
        and n_sp > 2
        and part % 16 == 0
        and width % (n_sp * 128) == 0
        and tokens % (n_sp * n_tp * 16) == 0
        and tokens * width <= 2**23
    )


def solution(mesh):
    in_specs = (
        P("sp", "tp"),
        P("sp", "tp"),
        P("sp", "tp"),
        P("sp", "tp"),
        P("sp", "tp"),
        P("tp"),
        P("tp"),
        P("tp", None),
        P("sp", "tp"),
        P(),
        P("sp", "tp"),
        P("sp", "tp"),
        P("tp", "sp"),
    )
    out_specs = P("sp", "tp")
    n_sp, n_tp = mesh.shape["sp"], mesh.shape["tp"]

    def layer(*args):
        shapes = (args[0].shape[0], args[10].shape[1], args[10].shape[0], args[5].shape[0])
        body = per_device
        if fits(n_sp, n_tp, shapes):
            body = functools.partial(split_hidden, n_sp, n_tp)
        return jax.shard_map(
            body, mesh=mesh, in_specs=in_specs, out_specs=out_specs, check_vma=False
        )(*args)

    return layer
```
